32 devices in a mesh: grp: 2 (over y), ep: 4 (over z), tp: 4 (over x, core).
Axes of the slice: x: 2, y: 2, z: 4, core: 2. Of those that a mesh axis runs over, the one named last changes fastest.
Arguments:
- queries: bfloat16 [4096, 512], P(('grp', 'ep'), 'tp'), parts along dimension 0, may hold values from -6 to 6
- keys: bfloat16 [4096, 512], P(('grp', 'ep'), 'tp'), parts along dimension 0, may hold values from -6 to 6
- values: bfloat16 [4096, 1024], P(('grp', 'ep'), 'tp'), parts along dimension 0, may hold values from -6 to 6
- gate: bfloat16 [4096, 1024], P(('grp', 'ep'), 'tp'), parts along dimension 0, may hold values from -6 to 6
- log_decay: float32 [4096, 8], P(('grp', 'ep'), 'tp'), parts along dimension 0, may hold values from -1 to 0, as said below
- w_out: bfloat16 [1024, 2048], P('tp'), may hold values from -0.1875 to 0.1875
- moe_input: bfloat16 [4096, 2048], P(('grp', 'ep', 'tp')), parts along dimension 0, may hold values from -40 to 40
- moe_gain: float32 [2048], replicated, may hold values from 0.1 to 1.9
- routes: int32 [4096, 2], P(('grp', 'ep', 'tp')), parts along dimension 0, may hold values from 0 to 15, all different within a row; in each aligned block of 128 rows (0 to 127, 128 to 255, ...) at most 24 rows name the same one
- route_weight: float32 [4096, 2], P(('grp', 'ep', 'tp')), parts along dimension 0, may hold values from 0.1 to 1
- expert_gate: bfloat16 [16, 2048, 512], P(('ep', 'tp')), may hold values from -0.125 to 0.125
- expert_up: bfloat16 [16, 2048, 512], P(('ep', 'tp')), may hold values from -0.125 to 0.125
- expert_down: bfloat16 [16, 512, 2048], P(('ep', 'tp')), may hold values from -0.25 to 0.25
- shared_gate: bfloat16 [2048, 512], P(None, 'tp'), may hold values from -0.125 to 0.125
- shared_up: bfloat16 [2048, 512], P(None, 'tp'), may hold values from -0.125 to 0.125
- shared_down: bfloat16 [512, 2048], P('tp'), may hold values from -0.25 to 0.25
Outputs:
- mixer_out: bfloat16 [4096, 2048], P(('grp', 'ep', 'tp')), parts along dimension 0
- moe_out: bfloat16 [4096, 2048], P(('grp', 'ep', 'tp')), parts along dimension 0
The draws below stay inside these ranges and needn't reach their ends.
There are 2 independent parts, one for each index of `grp`. The reference program is written for one: setup_inputs(seed, part) draws one part's arguments, and reference() takes and returns one part's arrays. A program takes and returns all parts, laid end to end along the dimension named above; an argument that names none is the same for every part. Nothing has to cross between parts.
Inputs may be any that keep to these rules, and one draw needn't show every extreme that they name: `routes`: each row names 2 different experts; in each aligned block of 128 rows (the rows of one device) no expert is named by more than 24 rows, a bound that some block reaches. `log_decay`: below zero.
All inputs are finite; a program needn't handle non-finite values.
Results may differ from the reference program's by a relative error of at most 0.015.
Values may be sent and summed in bfloat16 or wider, within the bound.
A program may use at most 128 MiB of HBM per device.

```python
import math
import jax
import jax.numpy as jnp
import numpy as np
from jax import lax

D = 2048
RETENTION_HEADS = 8
DK = 64
DV = 128
BLOCK = 128
FFE = 512
SH = 512
TOP = 2
TOK_DEV = 128
SPAN = 512
SEQUENCE_LENGTH = 2048
ROWS = 2048
EXPERTS = 16
CAP = 24
N_TP = 4


def draw_log_decay(key, part):
    parallel_flows = jax.random.split(key, 6)
    share = 0.5
    fast_head = jax.random.uniform(parallel_flows[0], (RETENTION_HEADS,)) < share
    reach_len = jnp.exp(jax.random.uniform(parallel_flows[1], (RETENTION_HEADS,), minval=math.log(30.0), maxval=math.log(100.0)))
    slow_rate = jax.random.uniform(parallel_flows[2], (RETENTION_HEADS,), minval=0.05, maxval=0.2) / SEQUENCE_LENGTH
    head_decay_rate = jnp.where(fast_head, math.log(10.0) / reach_len, slow_rate)
    decay_factor = jnp.exp(jax.random.uniform(parallel_flows[3], (SEQUENCE_LENGTH // SPAN, RETENTION_HEADS), minval=math.log(0.5), maxval=math.log(2.0)))
    decay_factor = jnp.repeat(decay_factor, SPAN, axis=0)
    expert_spike = jax.random.uniform(parallel_flows[4], (SEQUENCE_LENGTH, RETENTION_HEADS)) < 2.0 / SEQUENCE_LENGTH
    spike_penalty = jax.random.uniform(parallel_flows[5], (SEQUENCE_LENGTH, RETENTION_HEADS), minval=math.log(0.5), maxval=math.log(0.8))
    return (-head_decay_rate[None, :] * decay_factor + jnp.where(expert_spike, spike_penalty, 0.0)).astype(jnp.float32)


def draw_moe_input(key, part):
    parallel_flows = jax.random.split(key, 2)
    row_scale = jnp.exp(jax.random.uniform(parallel_flows[0], (ROWS, 1), minval=0.0, maxval=math.log(10.0)))
    base = jnp.clip(jax.random.normal(parallel_flows[1], (ROWS, D)), -4.0, 4.0)
    return (base * row_scale).astype(jnp.bfloat16)


def shard_levels(rng, extent, cuts, low, high):
    def one(dim, shards_of):
        steps = jax.random.uniform(jax.random.fold_in(jax.random.fold_in(rng, 6), dim), (shards_of,), jnp.float32, low / len(cuts), high / len(cuts))
        return jnp.repeat(jnp.exp(steps), extent[dim] // shards_of).reshape((-1,) + (1,) * (len(extent) - dim - 1))

    loudness = one(*cuts[0])
    for cut in cuts[1:]:
        loudness = loudness * one(*cut)
    return loudness


def shared_out(own_key, own, number, rows, count, top, reach, slope):
    sequence = jax.random.permutation(own_key, count)
    heavy_load, usual = load_shares(count, rows * top, reach, slope, True), load_shares(count, rows * top, reach, slope, False)
    places = jnp.arange(count)

    def named(sizes, offset_by):
        used = int((sizes > 0).sum())
        fixed = max(1, used // 4)
        shifted = fixed + (places - fixed + offset_by * (used - fixed)) % max(1, count - fixed)
        return jnp.zeros((count,), jnp.int32).at[sequence[jnp.where(places < fixed, places, shifted)]].set(jnp.asarray(sizes, jnp.int32))

    sizes = jnp.where(number % 4 == 0, named(heavy_load, number // 4), named(usual, number - number // 4 - 1))
    mixed = jax.random.permutation(jax.random.fold_in(own, 3), count)
    donor, sink = mixed[0:count // 2 * 2:2], mixed[1:count // 2 * 2:2]
    margin = jnp.minimum(sizes[donor] - 1, reach - sizes[sink]) // 2
    margin = jnp.where((donor == sequence[0]) | (sink == sequence[0]) | (sizes[sink] == 0), 0, jnp.maximum(margin, 0))
    shifted = jax.random.randint(jax.random.fold_in(own, 4), (count // 2,), 0, 1 << 20) % (margin + 1)
    sizes = sizes.at[donor].add(-shifted).at[sink].add(shifted)
    items = jnp.searchsorted(jnp.cumsum(sizes), jnp.arange(rows * top), side="right").astype(jnp.int32)
    listing = items.reshape(top, rows).T
    listing = listing[jax.random.permutation(jax.random.fold_in(own, 1), rows)]
    offset_by = jax.random.randint(jax.random.fold_in(own, 2), (rows, 1), 0, top)
    return jnp.take_along_axis(listing, (jnp.arange(top)[None, :] + offset_by) % top, axis=1)


def load_shares(amount, total, reach, lean, full):
    loads = [(1 << 20) // math.isqrt(grade ** lean) + 1 for grade in range(1, amount + 1)]
    largest = reach if full else min(reach, max(-(-total // amount), total * loads[0] // sum(loads)))
    least = 1 if total - largest >= amount - 1 else 0
    counts, spare = [largest] + [least] * (amount - 1), total - largest - least * (amount - 1)
    while spare > 0:
        movable = [i for i in range(1, amount) if counts[i] < largest] or [i for i in range(1, amount) if counts[i] < reach]
        whole, budget = sum([loads[i] for i in movable]), spare
        for i in movable:
            extra = min(reach - counts[i], max(1, budget * loads[i] // whole), spare)
            counts[i] = counts[i] + extra
            spare = spare - extra
    return np.array(counts)


def normal_values(rng, extent, scale, most, pieces=(), held_as=jnp.bfloat16):
    factor_of = shard_levels(rng, extent, pieces, -0.22, 0.18) if pieces else 1.0
    result = jax.random.normal(rng, extent, jnp.float32) * scale * factor_of
    return jnp.minimum(jnp.maximum(result, -most), most).astype(held_as)


def setup_inputs(seed: int = 0, part: int = 0) -> dict:
    key_list = jax.random.split(jax.random.key(seed), 17)
    part_keys = jax.random.split(jax.random.fold_in(key_list[16], part), 17)
    queries = normal_values(part_keys[0], (SEQUENCE_LENGTH, RETENTION_HEADS * DK), 1.0, 6.0, ((0, 4), (1, 4)))
    keys = normal_values(part_keys[1], (SEQUENCE_LENGTH, RETENTION_HEADS * DK), 1.0, 6.0, ((0, 4), (1, 4)))
    values = normal_values(part_keys[2], (SEQUENCE_LENGTH, RETENTION_HEADS * DV), 1.0, 6.0, ((0, 4), (1, 4)))
    gate = normal_values(part_keys[3], (SEQUENCE_LENGTH, RETENTION_HEADS * DV), 1.0, 6.0, ((0, 4), (1, 4)))
    log_decay = draw_log_decay(jax.random.fold_in(jax.random.fold_in(key_list[16], part), 71), part)
    w_out = normal_values(key_list[5], (RETENTION_HEADS * DV, D), (RETENTION_HEADS * DV) ** -0.5, 0.1875, ((0, 4),))
    moe_input = draw_moe_input(jax.random.fold_in(jax.random.fold_in(key_list[16], part), 71), part)
    moe_gain = jnp.clip(1.0 + 0.18 * jax.random.normal(key_list[7], (D,), jnp.float32), 0.1, 1.9)
    routes_keys = jax.random.split(jax.random.fold_in(part_keys[8], 1), ROWS // TOK_DEV)
    routes_turns = jax.random.permutation(jax.random.fold_in(part_keys[8], 3), ROWS // TOK_DEV)
    routes = jax.vmap(lambda own, number: shared_out(jax.random.fold_in(part_keys[8], 2), own, number, TOK_DEV, EXPERTS, TOP, CAP, 1))(routes_keys, routes_turns).reshape((ROWS, TOP))
    route_weight = jnp.clip(0.1 + 0.9 * jax.random.uniform(part_keys[9], (ROWS, TOP), jnp.float32) ** shard_levels(part_keys[9], (ROWS, TOP), ((0, 16),), -0.2, 0.2), 0.1, 1.0)
    expert_gate = normal_values(key_list[10], (EXPERTS, D, FFE), D ** -0.5, 0.125, ((0, 16),))
    expert_up = normal_values(key_list[11], (EXPERTS, D, FFE), D ** -0.5, 0.125, ((0, 16),))
    expert_down = normal_values(key_list[12], (EXPERTS, FFE, D), FFE ** -0.5, 0.25, ((0, 16),))
    shared_gate = normal_values(key_list[13], (D, SH), D ** -0.5, 0.125, ((1, 4),))
    shared_up = normal_values(key_list[14], (D, SH), D ** -0.5, 0.125, ((1, 4),))
    shared_down = normal_values(key_list[15], (SH, D), SH ** -0.5, 0.25, ((0, 4),))
    return dict(queries=queries, keys=keys, values=values, gate=gate, log_decay=log_decay, w_out=w_out, moe_input=moe_input, moe_gain=moe_gain, routes=routes, route_weight=route_weight, expert_gate=expert_gate, expert_up=expert_up, expert_down=expert_down, shared_gate=shared_gate, shared_up=shared_up, shared_down=shared_down)


ROPE_BASE = 10000.0
GROUP_EPS = 1e-05
NORM_EPS = 1e-06

def rotate(tensor, offset):
    half_dim = tensor.shape[-1] // 2
    frequency = ROPE_BASE ** (-jnp.arange(half_dim, dtype=jnp.float32) / half_dim)
    places = (offset + jnp.arange(tensor.shape[0], dtype=jnp.int32)).astype(jnp.float32)
    angles = places[:, None] * frequency[None, :]
    cosine = jnp.cos(angles)[:, None, :]
    sine_part = jnp.sin(angles)[:, None, :]
    as_float = tensor.astype(jnp.float32)
    first_half = as_float[..., :half_dim]
    second_half = as_float[..., half_dim:]
    return jnp.concatenate([first_half * cosine - second_half * sine_part, first_half * sine_part + second_half * cosine], axis=-1)

def block_step(carry_state, inputs):
    q_block, k_block, v_block, decay_block = inputs
    block_len = decay_block.shape[0]
    running = jnp.cumsum(decay_block, axis=0)
    total_log = running[-1]
    lower_mask = jnp.arange(block_len)[:, None] >= jnp.arange(block_len)[None, :]
    log_gap = jnp.transpose(running)[:, :, None] - jnp.transpose(running)[:, None, :]
    scores = jnp.einsum('ihd,jhd->hij', q_block.astype(jnp.float32), k_block.astype(jnp.float32))
    weights = jnp.where(lower_mask[None], scores * jnp.exp(jnp.where(lower_mask[None], log_gap, 0.0)), 0.0)
    weights = weights.astype(jnp.bfloat16)
    inner_out = jnp.einsum('hij,jhe->ihe', weights.astype(jnp.float32), v_block.astype(jnp.float32))
    lifted = q_block.astype(jnp.float32) * jnp.exp(running)[:, :, None]
    carried = jnp.einsum('ihd,hde->ihe', lifted, carry_state, precision=lax.Precision.HIGHEST)
    key_tail = k_block.astype(jnp.float32) * jnp.exp(total_log[None, :] - running)[:, :, None]
    carry_state = carry_state * jnp.exp(total_log)[:, None, None] + jnp.einsum('jhd,jhe->hde', key_tail, v_block.astype(jnp.float32), precision=lax.Precision.HIGHEST)
    return (carry_state, inner_out + carried)

def round_trip(tensor):
    return lax.optimization_barrier(tensor.astype(jnp.bfloat16)).astype(jnp.float32)

def reference(queries, keys, values, gate, log_decay, w_out, moe_input, moe_gain, routes, route_weight, expert_gate, expert_up, expert_down, shared_gate, shared_up, shared_down):
    q_rot = rotate(queries.reshape(SEQUENCE_LENGTH, RETENTION_HEADS, DK), 0).astype(jnp.bfloat16)
    k_rot = (rotate(keys.reshape(SEQUENCE_LENGTH, RETENTION_HEADS, DK), 0) * DK ** (-0.5)).astype(jnp.bfloat16)
    v_heads = values.reshape(SEQUENCE_LENGTH, RETENTION_HEADS, DV)
    blocks = SEQUENCE_LENGTH // BLOCK

    def to_blocks(tensor):
        return tensor.reshape((blocks, BLOCK) + tensor.shape[1:])
    zero_state = jnp.zeros((RETENTION_HEADS, DK, DV), jnp.float32)
    _, retained = lax.scan(block_step, zero_state, (to_blocks(q_rot), to_blocks(k_rot), to_blocks(v_heads), to_blocks(log_decay)))
    retained = retained.reshape(SEQUENCE_LENGTH, RETENTION_HEADS, DV)
    center = lax.optimization_barrier(jnp.mean(retained, axis=-1, keepdims=True))
    spread = lax.optimization_barrier(jnp.mean(jnp.square(retained - center), axis=-1, keepdims=True))
    normed = (retained - center) * lax.rsqrt(spread + GROUP_EPS)
    gate_act = jax.nn.silu(gate.astype(jnp.float32)).reshape(SEQUENCE_LENGTH, RETENTION_HEADS, DV)
    gated_out = (gate_act * normed).astype(jnp.bfloat16).reshape(SEQUENCE_LENGTH, RETENTION_HEADS * DV)
    group_cols = RETENTION_HEADS * DV // N_TP
    mixer_sum = jnp.zeros((SEQUENCE_LENGTH, D), jnp.float32)
    for member in range(N_TP):
        partial_value = jnp.dot(gated_out[:, member * group_cols:(member + 1) * group_cols], w_out[member * group_cols:(member + 1) * group_cols], preferred_element_type=jnp.float32)
        mixer_sum = mixer_sum + round_trip(partial_value)
    mixer_out = mixer_sum.astype(jnp.bfloat16)
    as_float = moe_input.astype(jnp.float32)
    scale_row = lax.rsqrt(lax.optimization_barrier(jnp.mean(as_float * as_float, axis=-1, keepdims=True)) + NORM_EPS)
    normed_rows = (as_float * scale_row * moe_gain.astype(jnp.float32)[None, :]).astype(jnp.bfloat16)
    shared_hidden = (jax.nn.silu(jnp.dot(normed_rows, shared_gate, preferred_element_type=jnp.float32)) * jnp.dot(normed_rows, shared_up, preferred_element_type=jnp.float32)).astype(jnp.bfloat16)
    unit_cols = SH // N_TP
    shared_sum = jnp.zeros((ROWS, D), jnp.float32)
    for member in range(N_TP):
        partial_value = jnp.dot(shared_hidden[:, member * unit_cols:(member + 1) * unit_cols], shared_down[member * unit_cols:(member + 1) * unit_cols], preferred_element_type=jnp.float32)
        shared_sum = shared_sum + round_trip(partial_value)
    pairs = ROWS * TOP
    sources = ROWS // TOK_DEV
    chosen = routes.reshape(pairs).astype(jnp.int32)
    marked = (chosen[:, None] == jnp.arange(EXPERTS, dtype=jnp.int32)[None, :]).astype(jnp.int32)
    counted = jnp.cumsum(marked.reshape(sources, TOK_DEV * TOP, EXPERTS), axis=1).reshape(pairs, EXPERTS)
    slot_rank = lax.optimization_barrier(jnp.sum(counted * marked, axis=1)) - 1
    owners = jnp.arange(pairs, dtype=jnp.int32) // (TOK_DEV * TOP)
    slots = ((owners * EXPERTS + chosen) * CAP + slot_rank).astype(jnp.int32)
    row_table = jnp.full((sources * EXPERTS * CAP,), ROWS, jnp.int32).at[slots].set(jnp.arange(pairs, dtype=jnp.int32) // TOP)
    weight_table = jnp.zeros((sources * EXPERTS * CAP,), jnp.float32).at[slots].set(route_weight.reshape(pairs).astype(jnp.float32))
    row_table = jnp.transpose(row_table.reshape(sources, EXPERTS, CAP), (1, 0, 2)).reshape(EXPERTS, sources * CAP)
    weight_table = jnp.transpose(weight_table.reshape(sources, EXPERTS, CAP), (1, 0, 2)).reshape(EXPERTS, sources * CAP)
    padded = jnp.concatenate([normed_rows, jnp.zeros((1, D), jnp.bfloat16)], axis=0)

    def expert_step(totals, inputs):
        rows_used, row_weights, gate_w, up_w, down_w = inputs
        picked = padded[rows_used]
        hidden = (jax.nn.silu(jnp.dot(picked, gate_w, preferred_element_type=jnp.float32)) * jnp.dot(picked, up_w, preferred_element_type=jnp.float32)).astype(jnp.bfloat16)
        answer = round_trip(jnp.dot(hidden, down_w, preferred_element_type=jnp.float32))
        return (totals.at[rows_used].add(answer * row_weights[:, None]), None)
    totals, _ = lax.scan(expert_step, jnp.zeros((ROWS + 1, D), jnp.float32), (row_table, weight_table, expert_gate, expert_up, expert_down))
    moe_out = (shared_sum + totals[:ROWS]).astype(jnp.bfloat16)
    return (mixer_out, moe_out)
```

```python
import functools

import jax
import jax.numpy as jnp
import numpy as np
from jax import lax
from jax.experimental import pallas as pl
from jax.experimental.pallas import tpu as pltpu
from jax.sharding import PartitionSpec as P

BLOCK = 128
ROPE_BASE = 10000.0
GROUP_EPS = 1e-05
NORM_EPS = 1e-06
DIRECT = 8
F32 = jnp.float32
BF16 = jnp.bfloat16


def swap(x, axis, bit):
    n = lax.axis_size(axis)
    return lax.ppermute(x, axis, [(i, i ^ bit) for i in range(n)])


def bits_of(n):
    assert n & (n - 1) == 0
    return [1 << i for i in range(n.bit_length() - 1)]


def gather_rel(x, axis):
    blocks = {0: x}
    for bit in reversed(bits_of(lax.axis_size(axis))):
        blocks.update({rel ^ bit: swap(blk, axis, bit) for rel, blk in list(blocks.items())})
    return blocks


def scatter_rel(parts, axis):
    parts = dict(parts)
    for bit in bits_of(lax.axis_size(axis)):
        for rel in [r for r in parts if r & bit]:
            got = swap(parts.pop(rel).astype(BF16), axis, bit)
            parts[rel ^ bit] = parts[rel ^ bit].astype(F32) + got.astype(F32)
    return parts[0]


def rope(x, angles, half):
    lanes = x.shape[1]
    row = lax.broadcasted_iota(jnp.int32, (lanes, lanes), 0)
    col = lax.broadcasted_iota(jnp.int32, (lanes, lanes), 1)
    low = (col % (2 * half)) < half
    turn = jnp.where(
        low & (row == col + half), -1.0, jnp.where((~low) & (row == col - half), 1.0, 0.0)
    ).astype(BF16)
    other = jnp.dot(x, turn, preferred_element_type=F32)
    return x.astype(F32) * jnp.cos(angles) + other * jnp.sin(angles)


def local_kernel(
    heads, q_ref, k_ref, v_ref, d_ref, a_ref, out_ref, lift_ref, state_ref, offset=None
):
    span, width = q_ref.shape
    dk = width // heads
    dv = v_ref.shape[1] // heads
    angles = a_ref[...]
    if offset is not None:
        place = offset + lax.broadcasted_iota(jnp.int32, (span, width), 0)
        angles = place.astype(F32) * angles
    q = rope(q_ref[...], angles, dk // 2).astype(BF16)
    k = (rope(k_ref[...], angles, dk // 2) * dk**-0.5).astype(BF16)
    row = lax.broadcasted_iota(jnp.int32, (BLOCK, BLOCK), 0)
    col = lax.broadcasted_iota(jnp.int32, (BLOCK, BLOCK), 1)
    lower = row >= col
    tri = lower.astype(F32)
    lane = lax.broadcasted_iota(jnp.int32, (BLOCK, width), 1)
    dlane = lax.broadcasted_iota(jnp.int32, (heads, width), 1)
    drow = lax.broadcasted_iota(jnp.int32, (heads, width), 0)
    spread = (dlane // dk == drow).astype(F32)
    state = [jnp.zeros((width, dv), F32) for _ in range(heads)]
    past = jnp.zeros((1, width), F32)
    for b in range(span // BLOCK):
        rows = pl.ds(b * BLOCK, BLOCK)
        at = slice(b * BLOCK, (b + 1) * BLOCK)
        qb, kb = q[at], k[at]
        wide = lax.dot_general(d_ref[:, rows], spread, (((0,), (0,)), ((), ())), precision=lax.Precision.HIGHEST,
                       preferred_element_type=F32)
        run = jnp.dot(tri, wide, precision=lax.Precision.HIGHEST, preferred_element_type=F32)
        last = run[BLOCK - 1 : BLOCK, :]
        lifted = (qb.astype(F32) * jnp.exp(run)).astype(BF16)
        lift_ref[rows, :] = (qb.astype(F32) * jnp.exp(run + past)).astype(BF16)
        tail = (kb.astype(F32) * jnp.exp(last - run)).astype(BF16)
        run_t = run.T
        for h in range(heads):
            mine = lane // dk == h
            zero = jnp.zeros((), BF16)
            qh = jnp.where(mine, qb, zero)
            vb = v_ref[rows, h * dv : (h + 1) * dv]
            scores = lax.dot_general(qh, kb, (((1,), (1,)), ((), ())), preferred_element_type=F32)
            gap = run[:, h * dk : h * dk + 1] - run_t[h * dk : h * dk + 1, :]
            w = jnp.where(lower, scores * jnp.exp(jnp.where(lower, gap, 0.0)), 0.0).astype(BF16)
            out = jnp.dot(w, vb, preferred_element_type=F32)
            if b:
                lh = jnp.where(mine, lifted, zero)
                out = out + jnp.dot(lh, state[h].astype(BF16), preferred_element_type=F32)
            out_ref[rows, h * dv : (h + 1) * dv] = out
            th = jnp.where(mine, tail, zero)
            grown = lax.dot_general(th, vb, (((0,), (0,)), ((), ())), preferred_element_type=F32)
            state[h] = state[h] * jnp.exp(last[:, h * dk : h * dk + 1]) + grown
        past = past + last
    total = state[0]
    for h in range(1, heads):
        total = total + state[h]
    state_ref[:width, :] = total.astype(BF16)
    hi = past.astype(BF16)
    lo = (past - hi.astype(F32)).astype(BF16)
    pad = 8
    state_ref[width : width + pad, :] = jnp.broadcast_to(hi, (pad, width))
    state_ref[width + pad :, :] = jnp.broadcast_to(lo, (pad, width))


def finish_kernel(heads, out_ref, lift_ref, state_ref, gate_ref, w_ref, mix_ref):
    width = lift_ref.shape[1]
    dk = width // heads
    dv = out_ref.shape[1] // heads
    lane = lax.broadcasted_iota(jnp.int32, (BLOCK, width), 1)

    def one(b, carry):
        rows = pl.ds(pl.multiple_of(b * BLOCK, BLOCK), BLOCK)
        lift = lift_ref[rows, :]
        total = jnp.zeros((BLOCK, w_ref.shape[1]), F32)
        for h in range(heads):
            lh = jnp.where(lane // dk == h, lift, jnp.zeros((), BF16))
            r = out_ref[rows, h * dv : (h + 1) * dv] + jnp.dot(
                lh, state_ref[...], preferred_element_type=F32
            )
            r = r - jnp.mean(r, axis=-1, keepdims=True)
            r = r * lax.rsqrt(jnp.mean(r * r, axis=-1, keepdims=True) + GROUP_EPS)
            g = gate_ref[rows, h * dv : (h + 1) * dv].astype(F32)
            y = (g * jax.nn.sigmoid(g) * r).astype(BF16)
            total = total + jnp.dot(
                y, w_ref[h * dv : (h + 1) * dv, :], preferred_element_type=F32
            )
        mix_ref[rows, :] = total.astype(BF16)
        return carry

    lax.fori_loop(0, out_ref.shape[0] // BLOCK, one, 0)


def call(kernel, out_shape, flops, moved, *args):
    vmem = pl.BlockSpec(memory_space=pltpu.VMEM)
    return pl.pallas_call(
        kernel,
        out_shape=out_shape,
        in_specs=[vmem] * len(args),
        out_specs=jax.tree.map(lambda _: vmem, out_shape),
        cost_estimate=pl.CostEstimate(flops=flops, bytes_accessed=moved, transcendentals=0),
        compiler_params=pltpu.CompilerParams(vmem_limit_bytes=32 << 20),
    )(*args)


def semaphores(cuts, subs):
    sizes = dict(
        meta=3, rows=5, state=3, near=2, fmeta=4, mix=2, mix2=cuts, nback=2 * cuts,
        first=2 * cuts, second=cuts, dense=4 * subs, far=8 * subs, back=16 * subs,
        pass_on=4 * subs, fin=2 * subs,
    )
    base, total = {}, 0
    for name, size in sizes.items():
        base[name] = total
        total += size
    return base, total


SENDS = 192


class At:
    def __init__(self, ref):
        self.ref = ref

    def __getitem__(self, index):
        return self.ref, index


def mega_kernel(
    dims,
    q_ref, k_ref, v_ref, gate_ref, d_ref, f_ref, x_ref, gain_ref, route_ref, weigh_ref,
    wo_hbm, eg_hbm, eu_hbm, ed_hbm, sg_hbm, su_hbm, sd_hbm,
    mix_out, moe_out,
    lout, lift, spack, srecv, nbuf, mbuf, fmeta, fbuf, pfar, afar, yfar, pass_buf, ycomb, dsend, fin,
    wfar, pfar_pick, stbuf, psendn, parrn, ysendn, yrecv, wbuf, hbuf,
    mpart, mrecv, opart, orecv, wo, eg, eu, ed, sg, su, sd,
    send_sem, recv_sem, local_sem,
):
    heads, ep_n, tp_n, cap, top, cuts, subs = dims
    z, t = lax.axis_index("ep"), lax.axis_index("tp")
    rows, model = x_ref.shape
    span, width = q_ref.shape
    piece = model // cuts
    part_w = model // (2 * subs)
    pair = 2 * cap
    half_n = tp_n // 2
    bits = bits_of(tp_n)
    sems, _ = semaphores(cuts, subs)

    core = lax.rem(t, 2)
    cx = [core, 1 - core]
    line = t - core
    tps = [t, line + 1 - core, tp_n - 2 - line + core, tp_n - 1 - t]
    ends = [line, line + 1]
    side = z // 2
    near = z + 1 - 2 * lax.rem(z, 2)
    inner = (z == 1) | (z == 2)
    outer = jnp.logical_not(inner)
    relay = 2 - side
    beyond = 3 - 3 * side
    near_peer = {"ep": near}
    crossing = {"ep": relay}

    mbuf[0, :top, :] = route_ref[...].astype(F32)
    mbuf[0, top : 2 * top, :] = weigh_ref[...]
    mbuf[0, 2 * top :, :] = jnp.zeros((8 - 2 * top, rows), F32)
    loads = []
    for i, (a, b) in enumerate(
        ((sg_hbm, sg), (su_hbm, su), (eg_hbm.at[0], eg), (eu_hbm.at[0], eu),
         (ed_hbm.at[0], ed), (wo_hbm, wo), (sd_hbm, sd))
    ):
        loads.append(pltpu.make_async_copy(a, b, local_sem.at[i]))
        loads[-1].start()

    barrier = pltpu.get_barrier_semaphore()
    for s in range(ep_n):
        for r in range(tp_n):
            if s or r:
                pl.semaphore_signal(
                    barrier, 1, device_id={"ep": lax.rem(z + s, ep_n), "tp": tps[r]}
                )

    src = x_ref[...].astype(F32)
    scale = lax.rsqrt(jnp.mean(src * src, axis=-1, keepdims=True) + NORM_EPS)
    nbuf[:rows, :] = (src * scale * gain_ref[...]).astype(BF16)
    for s in range(1, ep_n):
        @pl.when(z < s)
        def _():
            srecv[s] = jnp.zeros(srecv.shape[1:], BF16)
    pl.semaphore_wait(barrier, ep_n * tp_n - 1)

    started = []

    def describe(k, i, src, dst, peer):
        src, dst = (r[0].at[r[1]] if isinstance(r, tuple) else r for r in (src, dst))
        return pltpu.make_async_remote_copy(
            src_ref=src, dst_ref=dst, send_sem=send_sem.at[k], recv_sem=recv_sem.at[i],
            device_id=peer,
        )

    def go(i, src, dst, peer, who=None):
        job = (len(started), i, src, dst, peer)
        describe(*job).start()
        started.append((job, who))

    def arrived(i, dst):
        describe(0, i, dst, dst, near_peer).wait_recv()

    def block(rel):
        return pl.ds(rel * rows, rows)

    def send_dense(f, sub, who):
        for ch in range(2):
            cols = pl.ds((ch * subs + sub) * part_w, part_w)
            go(
                dense_sem[f][sub], At(nbuf)[block(0), cols], At(fbuf)[f, sub, own_rows],
                {"ep": relay, "tp": ends[ch]}, who,
            )

    own_rows = pl.ds(pl.multiple_of(core * rows, rows), rows)
    dense_sem = [
        [sems["dense"] + 2 * f * subs + core * subs + sub for sub in range(subs)] for f in range(2)
    ]
    fmeta_sem = [sems["fmeta"] + 2 * f + core for f in range(2)]
    mine = [core * subs + sub for sub in range(subs)]
    fin_sem = [sems["fin"] + m for m in mine]
    cross = [[cx[c] * subs + sub for sub in range(subs)] for c in range(2)]
    one, two = {"tp": tps[1]}, {"tp": tps[2]}

    go(sems["meta"], At(mbuf)[0], At(mbuf)[1], one)
    go(sems["rows"], At(nbuf)[block(0)], At(nbuf)[block(1)], one)
    go(sems["meta"] + 1, At(mbuf)[0], At(mbuf)[2], two)
    halves = [pl.ds(h * (model // 2), model // 2) for h in range(2)]
    for h in range(2):
        go(sems["rows"] + 1 + h, At(nbuf)[block(0), halves[h]], At(nbuf)[block(2), halves[h]], two)
    for f, here in ((0, inner), (1, outer)):
        @pl.when(here)
        def _():
            for ch in range(2):
                go(
                    fmeta_sem[f], At(mbuf)[0], At(fmeta)[f, core],
                    {"ep": relay, "tp": ends[ch]}, here,
                )
            if f == 1:
                send_dense(f, 0, here)

    lane = lax.broadcasted_iota(jnp.int32, (rows, rows), 1)
    sub_i = lax.broadcasted_iota(jnp.int32, (rows, rows), 0)
    before = (sub_i < lane).astype(BF16)
    slot_id = lax.broadcasted_iota(jnp.int32, (cap, rows), 0).astype(F32)
    blank = jnp.zeros((cap, rows), F32)
    index = lax.broadcasted_iota(jnp.int32, (8, rows), 0)

    def plan(metas, experts):
        names = jnp.full((8, rows), -1, jnp.int32)
        for i, e in enumerate(experts):
            names = jnp.where(index == i, e, names)
        names = names.astype(F32)
        ranks, weights = [], []
        for m in metas:
            hit = [m[k : k + 1, :] == names for k in range(top)]
            mark = functools.reduce(jnp.logical_or, hit)
            weights.append(
                sum(jnp.where(hit[k], m[top + k : top + k + 1, :], 0.0) for k in range(top))
            )
            rank = jnp.dot(
                mark.astype(F32).astype(BF16), before, preferred_element_type=F32
            )
            ranks.append(jnp.where(mark, rank, -1.0))
        picks, scaled = [], []
        for i in range(len(experts)):
            for s in range(2):
                at = jnp.where(slot_id == ranks[s][i : i + 1, :], 1.0, 0.0)
                heavy = at * weights[s][i : i + 1, :]
                picks.append(jnp.concatenate([blank, at] if s else [at, blank], axis=1))
                scaled.append(jnp.concatenate([blank, heavy] if s else [heavy, blank], axis=1))
        return (
            jnp.concatenate(picks, axis=0).astype(BF16),
            jnp.concatenate(scaled, axis=0).astype(BF16),
        )

    def route(g):
        pick, scaled = plan(
            [mbuf[2 * g], mbuf[2 * g + 1]], [z * tp_n + t, near * tp_n + t]
        )
        wbuf[g] = scaled
        sent = jnp.dot(
            pick, nbuf[2 * g * rows : (2 * g + 2) * rows, :], preferred_element_type=F32
        ).astype(BF16)
        psendn[g] = sent[pair:]
        parrn[0, g] = sent[:pair]
        go(sems["near"] + g, At(psendn)[g], At(parrn)[1, g], near_peer)

    def first_rows():
        arrived(sems["meta"], At(mbuf)[1])
        arrived(sems["rows"], At(nbuf)[block(1)])
        route(0)

    def early_dense(sub):
        @pl.when(inner)
        def _():
            send_dense(0, sub, inner)

    def late_dense(sub):
        @pl.when(outer)
        def _():
            send_dense(1, sub, outer)

    def local():
        local_kernel(heads, q_ref, k_ref, v_ref, d_ref, f_ref, lout, lift, spack, z * span)
        for s in range(1, ep_n):
            later = z + s < ep_n
            after = {"ep": lax.rem(z + s, ep_n)}

            @pl.when(later)
            def _():
                go(sems["state"] + s - 1, spack, At(srecv)[s], after, later)

    def shared(j):
        if j == 0:
            loads[0].wait()
            loads[1].wait()
        x = nbuf[block(j), :]
        g = jnp.dot(x, sg[...], preferred_element_type=F32)
        u = jnp.dot(x, su[...], preferred_element_type=F32)
        hbuf[block(j), :] = (g * jax.nn.sigmoid(g) * u).astype(BF16)

    def gather_states():
        for s in range(1, ep_n):
            @pl.when(z >= s)
            def _():
                arrived(sems["state"] + s - 1, At(srecv)[s])
        state_in = jnp.zeros((width, width), F32)
        since = jnp.zeros((8, width), F32)
        for s in range(1, ep_n):
            got = srecv[s].astype(F32)
            state_in = state_in + jnp.exp(since).T[:, :1] * got[:width]
            since = since + (got[width : width + 8] + got[width + 8 :])
        stbuf[...] = state_in.astype(BF16)
        loads[5].wait()

    def peer_of(j):
        peer = t
        for bit in bits:
            on = lax.rem(j // bit, 2)
            peer = peer + on * (bit - 2 * bit * lax.rem(t // bit, 2))
        return peer

    def finish(first):
        def one_block(i, c):
            j = 2 * i + first
            own = pl.multiple_of(peer_of(j) * (span // tp_n), BLOCK)
            finish_rows(
                heads, lout, lift, stbuf[...], gate_ref, wo, pl.ds(own, span // tp_n), mpart, j
            )
            return c

        lax.fori_loop(0, half_n, one_block, 0)
        if first:
            for i in range(half_n):
                go(sems["mix"] + i, At(mpart)[2 * i + 1], At(mrecv)[i], one)

    def second_rows(h):
        if h == 0:
            arrived(sems["meta"] + 1, At(mbuf)[2])
            go(sems["meta"] + 2, At(mbuf)[2], At(mbuf)[3], one)
        arrived(sems["rows"] + 1 + h, At(nbuf)[block(2), halves[h]])
        go(sems["rows"] + 3 + h, At(nbuf)[block(2), halves[h]], At(nbuf)[block(3), halves[h]], one)

    def mix_add():
        for i in reversed(range(half_n)):
            arrived(sems["mix"] + i, At(mrecv)[i])
            mpart[2 * i] = (mpart[2 * i].astype(F32) + mrecv[i].astype(F32)).astype(BF16)

    def mix_piece(c, who=None):
        cols = pl.ds(c * piece, piece)
        go(sems["mix2"] + c, At(mpart)[2, :, cols], At(mrecv)[half_n, :, cols], two, who)

    def mix_inner(c):
        pl.when(inner)(lambda: mix_piece(c, inner))

    def mix_outer(c):
        pl.when(outer)(lambda: mix_piece(c, outer))

    def mix_done():
        for c in range(cuts):
            arrived(sems["mix2"] + c, At(mrecv)[half_n, :, pl.ds(c * piece, piece)])
        mix_out[...] = (mpart[0].astype(F32) + mrecv[half_n].astype(F32)).astype(BF16)

    def third_rows():
        arrived(sems["meta"] + 2, At(mbuf)[3])
        for h in range(2):
            arrived(sems["rows"] + 3 + h, At(nbuf)[block(3), halves[h]])
        route(1)

    everyone = [
        (near if i // tp_n else z) * tp_n + tps[i % tp_n] for i in range(2 * tp_n)
    ]

    def plan_far(f):
        @pl.when(inner)
        def _():
            for s in range(2):
                arrived(sems["fmeta"] + 2 * f + s, At(fmeta)[f, s])
            pick, scaled = plan([fmeta[f, 0], fmeta[f, 1]], everyone)
            wfar[f] = scaled
            pfar_pick[f] = pick

    def relay_far(f, sub):
        @pl.when(inner)
        def _():
            for s in range(2):
                arrived(sems["dense"] + (2 * f + s) * subs + sub, At(fbuf)[f, sub, block(s)])
            pfar[f, sub] = jnp.dot(
                pfar_pick[f], fbuf[f, sub], preferred_element_type=F32
            ).astype(BF16)
            for i in (6, 7, 4, 5, 2, 3, 1):
                rel = i % tp_n
                go(
                    sems["far"] + (f * subs + sub) * tp_n + rel,
                    At(pfar)[f, sub, pl.ds(i * pair, pair)],
                    At(afar)[f, mine[sub], pl.ds((rel // 2) * pair, pair)],
                    {"ep": near if i // tp_n else z, "tp": tps[rel]}, inner,
                )
            afar[f, mine[sub], :pair] = pfar[f, sub, :pair]

    def hidden(x):
        g = jnp.dot(x, eg[...], preferred_element_type=F32)
        u = jnp.dot(x, eu[...], preferred_element_type=F32)
        return (g * jax.nn.sigmoid(g) * u).astype(BF16)

    def weights():
        for i in (2, 3, 4):
            loads[i].wait()

    def experts_near():
        for g in range(2):
            arrived(sems["near"] + g, At(parrn)[1, g])
        h = hidden(jnp.concatenate([parrn[s, g] for s in range(2) for g in range(2)], axis=0))
        for c in range(cuts):
            at = slice(c * piece, (c + 1) * piece)
            cols = pl.ds(c * piece, piece)
            y = jnp.dot(h, ed[:, at], preferred_element_type=F32).astype(BF16)
            ysendn[:, at] = y[2 * pair :]
            for g in range(2):
                yrecv[g, :pair, at] = y[g * pair : (g + 1) * pair]
                go(
                    sems["nback"] + 2 * c + g, At(ysendn)[pl.ds(g * pair, pair), cols],
                    At(yrecv)[g, pl.ds(pair, pair), cols], near_peer,
                )

    def experts_far(f):
        for sub in range(subs):
            for rel in range(tp_n):
                i = sems["far"] + (f * subs + sub) * tp_n + rel
                dst = At(afar)[f, cross[rel % 2][sub], pl.ds((rel // 2) * pair, pair)]
                if rel:
                    arrived(i, dst)
                else:
                    @pl.when(outer)
                    def _():
                        arrived(i, dst)
        h = hidden(jnp.concatenate([afar[f, q] for q in range(2 * subs)], axis=1))
        for sub in range(subs):
            for ch in range(2):
                q = ch * subs + sub
                yfar[f, q] = jnp.dot(
                    h, ed[:, q * part_w : (q + 1) * part_w], preferred_element_type=F32
                ).astype(BF16)
            base = sems["back"] + (f * subs + sub) * 2 * tp_n

            @pl.when(inner)
            def _():
                for rel in (2, 3, 1):
                    go(
                        base + rel,
                        At(yfar)[f, cross[rel % 2][sub], pl.ds((rel // 2) * pair, pair)],
                        At(ycomb)[f, sub, pl.ds(rel * pair, pair)], {"tp": tps[rel]}, inner,
                    )
                ycomb[f, sub, :pair] = yfar[f, mine[sub], :pair]

            @pl.when(outer)
            def _():
                for ch in range(2):
                    q = ch * subs + sub
                    go(
                        sems["pass_on"] + f * 2 * subs + q,
                        At(yfar)[f, q, pl.ds(pair, pair)], At(pass_buf)[f, q], two, outer,
                    )
                for c in range(2):
                    go(
                        base + tp_n + c, At(yfar)[f, cross[c][sub], pl.ds(0, pair)],
                        At(ycomb)[f, sub, pl.ds((tp_n + c) * pair, pair)],
                        {"ep": near, "tp": tps[c]}, outer,
                    )

    def pass_far(f, sub):
        @pl.when(outer)
        def _():
            for ch in range(2):
                q = ch * subs + sub
                arrived(sems["pass_on"] + f * 2 * subs + q, At(pass_buf)[f, q])
            for c in range(2):
                go(
                    sems["back"] + (f * subs + sub) * 2 * tp_n + tp_n + 2 + c,
                    At(pass_buf)[f, cross[c][sub]],
                    At(ycomb)[f, sub, pl.ds((tp_n + 2 + c) * pair, pair)],
                    {"ep": near, "tp": tps[c]}, outer,
                )

    def combine_far(f, sub):
        @pl.when(inner)
        def _():
            for i in range(1, 2 * tp_n):
                arrived(
                    sems["back"] + (f * subs + sub) * 2 * tp_n + i,
                    At(ycomb)[f, sub, pl.ds(i * pair, pair)],
                )
            dsend[f, sub] = lax.dot_general(
                wfar[f], ycomb[f, sub], (((0,), (0,)), ((), ())), preferred_element_type=F32
            ).astype(BF16)
            for s in range(2):
                go(
                    fin_sem[sub], At(dsend)[f, sub, block(s)], At(fin)[mine[sub]],
                    {"ep": beyond if f else relay, "tp": ends[s]}, inner,
                )

    def combine_near(c):
        if c == 0:
            loads[6].wait()
        at = slice(c * piece, (c + 1) * piece)
        cols = pl.ds(c * piece, piece)
        for g in range(2):
            arrived(sems["nback"] + 2 * c + g, At(yrecv)[g, pl.ds(pair, pair), cols])
        for g in (1, 0):
            part = lax.dot_general(
                wbuf[g], yrecv[g, :, at], (((0,), (0,)), ((), ())), preferred_element_type=F32
            )
            part = part + jnp.dot(
                hbuf[2 * g * rows : (2 * g + 2) * rows, :], sd[:, at], preferred_element_type=F32
            )
            opart[2 * g + 1, :, at] = part[rows:].astype(BF16)
            go(
                sems["first"] + 2 * c + g, At(opart)[2 * g + 1, :, cols],
                At(orecv)[g, :, cols], one,
            )
            opart[2 * g, :, at] = part[:rows].astype(BF16)

    def second(c):
        at = slice(c * piece, (c + 1) * piece)
        cols = pl.ds(c * piece, piece)
        for g in (1, 0):
            arrived(sems["first"] + 2 * c + g, At(orecv)[g, :, cols])
            opart[2 * g, :, at] = (
                opart[2 * g, :, at].astype(F32) + orecv[g, :, at].astype(F32)
            ).astype(BF16)
            if g:
                go(sems["second"] + c, At(opart)[2, :, cols], At(orecv)[2, :, cols], two)

    def moe_done():
        for c in range(cuts):
            arrived(sems["second"] + c, At(orecv)[2, :, pl.ds(c * piece, piece)])
        for sub in range(subs):
            for ch in range(2):
                q = ch * subs + sub
                at = slice(q * part_w, (q + 1) * part_w)
                arrived(sems["fin"] + q, At(fin)[q])
                moe_out[:, at] = (
                    opart[0, :, at].astype(F32) + orecv[2, :, at].astype(F32)
                    + fin[q].astype(F32)
                ).astype(BF16)

    local()
    early_dense(0)
    early_dense(1)
    first_rows()
    plan_far(1)
    shared(0)
    shared(1)
    relay_far(1, 0)
    second_rows(0)
    late_dense(1)
    gather_states()
    finish(1)
    finish(0)
    mix_add()
    mix_outer(0)
    mix_outer(1)
    mix_inner(0)
    mix_inner(1)
    second_rows(1)
    third_rows()
    relay_far(1, 1)
    plan_far(0)
    relay_far(0, 0)
    weights()
    experts_far(1)
    pass_far(1, 0)
    pass_far(1, 1)
    relay_far(0, 1)
    experts_near()
    mix_outer(2)
    mix_outer(3)
    mix_inner(2)
    mix_inner(3)
    shared(2)
    shared(3)
    experts_far(0)
    combine_far(1, 0)
    combine_far(1, 1)
    pass_far(0, 0)
    pass_far(0, 1)
    combine_near(0)
    combine_near(1)
    second(0)
    combine_near(2)
    second(1)
    combine_near(3)
    second(2)
    second(3)
    combine_far(0, 0)
    combine_far(0, 1)
    mix_done()
    moe_done()

    for job, who in started:
        if who is None:
            describe(*job).wait_send()
    conditions = []
    for _, who in started:
        if who is not None and all(who is not w for w in conditions):
            conditions.append(who)
    for w in conditions:
        @pl.when(w)
        def _():
            for job, who in started:
                if who is w:
                    describe(*job).wait_send()
    assert len(started) <= SENDS


def finish_rows(heads, lout, lift_ref, state, gate_ref, wo, at, mpart, j):
    width = lift_ref.shape[1]
    dk = width // heads
    dv = lout.shape[1] // heads
    lift = lift_ref[at, :]
    lane = lax.broadcasted_iota(jnp.int32, lift.shape, 1)
    ys = []
    for h in range(heads):
        lh = jnp.where(lane // dk == h, lift, jnp.zeros((), BF16))
        r = lout[at, h * dv : (h + 1) * dv] + jnp.dot(lh, state, preferred_element_type=F32)
        r = r - jnp.mean(r, axis=-1, keepdims=True)
        r = r * lax.rsqrt(jnp.mean(r * r, axis=-1, keepdims=True) + GROUP_EPS)
        g = gate_ref[at, h * dv : (h + 1) * dv].astype(F32)
        ys.append((g * jax.nn.sigmoid(g) * r).astype(BF16))
    y = jnp.concatenate(ys, axis=1)
    mpart[j] = jnp.dot(y, wo[...], preferred_element_type=F32).astype(BF16)


def mega(
    queries, keys, values, gate, log_decay, w_out, moe_input, moe_gain, routes, route_weight,
    expert_gate, expert_up, expert_down, shared_gate, shared_up, shared_down,
):
    span, width = queries.shape
    heads = log_decay.shape[1]
    half = width // heads // 2
    rows, model = moe_input.shape
    top = routes.shape[1]
    ep_n, tp_n = lax.axis_size("ep"), lax.axis_size("tp")
    cap = rows * top * 3 // (2 * ep_n * tp_n)
    pair, cuts, subs = 2 * cap, 4, 2
    steps = np.arange(half, dtype=np.float32) / np.float32(half)
    freq = np.power(np.float32(ROPE_BASE), -steps).astype(np.float32)
    freq = jnp.asarray(np.tile(freq, width // half)[None, :])
    vmem = pl.BlockSpec(memory_space=pltpu.VMEM)
    hbm = pl.BlockSpec(memory_space=pl.ANY)
    V = pltpu.VMEM
    half_n = tp_n // 2
    part_w = model // (2 * subs)
    copies = semaphores(cuts, subs)[1]
    results = pl.pallas_call(
        functools.partial(mega_kernel, (heads, ep_n, tp_n, cap, top, cuts, subs)),
        out_shape=(jax.ShapeDtypeStruct((rows, w_out.shape[1]), BF16),
                   jax.ShapeDtypeStruct((rows, model), BF16)),
        in_specs=[vmem] * 10 + [hbm] * 7,
        out_specs=(vmem, vmem),
        scratch_shapes=[
            V((span, values.shape[1]), F32), V((span, width), BF16),
            V((width + 16, width), BF16), V((ep_n, width + 16, width), BF16),
            V((tp_n * rows, model), BF16), V((tp_n, 8, rows), F32),
            V((2, 2, 8, rows), F32), V((2, subs, 2 * rows, part_w), BF16),
            V((2, subs, 2 * tp_n * pair, part_w), BF16), V((2, 2 * subs, 2 * pair, part_w), BF16),
            V((2, 2 * subs, 2 * pair, part_w), BF16), V((2, 2 * subs, pair, part_w), BF16),
            V((2, subs, 2 * tp_n * pair, part_w), BF16), V((2, subs, 2 * rows, part_w), BF16),
            V((2 * subs, rows, part_w), BF16), V((2, 2 * tp_n * pair, 2 * rows), BF16),
            V((2, 2 * tp_n * pair, 2 * rows), BF16), V((width, width), BF16),
            V((2, pair, model), BF16), V((2, 2, pair, model), BF16),
            V((2 * pair, model), BF16), V((2, 2 * pair, model), BF16),
            V((2, 2 * pair, 2 * rows), BF16), V((tp_n * rows, shared_gate.shape[1]), BF16),
            V((tp_n, span // tp_n, w_out.shape[1]), BF16),
            V((half_n + 1, span // tp_n, w_out.shape[1]), BF16),
            V((tp_n, rows, model), BF16), V((half_n + 1, rows, model), BF16),
            V(w_out.shape, BF16), V(expert_gate.shape[1:], BF16), V(expert_up.shape[1:], BF16),
            V(expert_down.shape[1:], BF16), V(shared_gate.shape, BF16),
            V(shared_up.shape, BF16), V(shared_down.shape, BF16),
            pltpu.SemaphoreType.DMA((SENDS,)), pltpu.SemaphoreType.DMA((copies,)),
            pltpu.SemaphoreType.DMA((7,)),
        ],
        compiler_params=pltpu.CompilerParams(
            collective_id=0, has_side_effects=True, vmem_limit_bytes=60 << 20
        ),
    )(
        queries, keys, values, gate, log_decay.T, freq, moe_input, moe_gain[None, :],
        routes.T, route_weight.T,
        w_out, expert_gate, expert_up, expert_down, shared_gate, shared_up, shared_down,
    )
    steps = 4 if rows % 64 == 0 else 1
    tile = pl.BlockSpec((rows // steps, model), lambda i: (i, 0))
    return pl.pallas_call(
        hand_over,
        grid=(steps,),
        out_shape=tuple(jax.ShapeDtypeStruct(r.shape, r.dtype) for r in results),
        in_specs=[tile] * 2,
        out_specs=(tile, tile),
    )(*results)


def hand_over(a_ref, b_ref, mix_ref, moe_ref):
    mix_ref[...] = a_ref[...]
    moe_ref[...] = b_ref[...]


def per_device(
    queries, keys, values, gate, log_decay, w_out, moe_input, moe_gain, routes, route_weight,
    expert_gate, expert_up, expert_down, shared_gate, shared_up, shared_down,
):
    span = queries.shape[0]
    heads = log_decay.shape[1]
    width = queries.shape[1]
    dk = width // heads
    half = dk // 2
    dv = values.shape[1] // heads
    rows, model = moe_input.shape
    top = routes.shape[1]
    ep_n, tp_n = lax.axis_size("ep"), lax.axis_size("tp")
    z, t = lax.axis_index("ep"), lax.axis_index("tp")
    direct = ep_n <= DIRECT and ep_n & (ep_n - 1) == 0
    if ep_n == 4 and tp_n == 4 and dv == width and (rows * top * 3 // (ep_n * tp_n)) % 16 == 0:
        return mega(
            queries, keys, values, gate, log_decay, w_out, moe_input, moe_gain, routes,
            route_weight, expert_gate, expert_up, expert_down, shared_gate, shared_up, shared_down,
        )
    cap = rows * top * 3 // (2 * ep_n * tp_n)

    source = moe_input.astype(F32)
    scale_row = lax.rsqrt(jnp.mean(source * source, axis=-1, keepdims=True) + NORM_EPS)
    normed = (source * scale_row * moe_gain[None, :]).astype(BF16)
    meta = jnp.concatenate([routes.astype(F32).T, route_weight.T], axis=0)
    blocks = gather_rel(normed, "tp")
    metas = gather_rel(meta, "tp")
    order = sorted(blocks)

    step = jnp.arange(ep_n, dtype=jnp.int32)
    peers = (z ^ step) if direct else step
    named = (peers * tp_n + t).astype(F32)
    before = (jnp.arange(rows)[:, None] < jnp.arange(rows)[None, :]).astype(BF16)
    parcels, weights = {}, {}
    for j in order:
        hits = metas[j][:top, None, :] == named[None, :, None]
        mark = jnp.any(hits, axis=0)
        weight = jnp.sum(jnp.where(hits, metas[j][top:, None, :], 0.0), axis=0)
        rank = jnp.dot(mark.astype(BF16), before, preferred_element_type=F32)
        slot = mark[:, None, :] & (rank[:, None, :] == jnp.arange(cap, dtype=F32)[None, :, None])
        pick = slot.astype(BF16).reshape(ep_n * cap, rows)
        weights[j] = jnp.where(slot, weight[:, None, :], 0.0).astype(BF16)
        parcels[j] = jnp.dot(pick, blocks[j], preferred_element_type=F32).astype(BF16).reshape(
            ep_n, cap, model
        )

    half_tp = max(1, tp_n // 2)
    groups = [order[:half_tp], order[half_tp:]] if tp_n > 1 else [order]

    def expert(x):
        g = jnp.dot(x, expert_gate[0], preferred_element_type=F32)
        u = jnp.dot(x, expert_up[0], preferred_element_type=F32)
        h = (jax.nn.silu(g) * u).astype(BF16)
        return jnp.dot(h, expert_down[0], preferred_element_type=F32).astype(BF16)

    cuts = 2
    piece = model // cuts
    answers = {}
    if direct:
        arrived = {}
        for group in groups:
            part = jnp.stack([parcels[j] for j in group], axis=1)
            for s in reversed(range(ep_n)):
                got = swap(part[s], "ep", s) if s else part[0]
                arrived.setdefault(s, []).append(got)
        for s in reversed(range(ep_n)):
            flat = jnp.concatenate(arrived[s], axis=0).reshape(tp_n * cap, model)
            y = expert(flat)
            for c in range(cuts):
                back = y[:, c * piece : (c + 1) * piece]
                answers[c, s] = (swap(back, "ep", s) if s else back).reshape(tp_n, cap, piece)
        answers = {
            c: jnp.stack([answers[c, s] for s in range(ep_n)], axis=1) for c in range(cuts)
        }
    else:
        part = jnp.stack([parcels[j] for j in order], axis=1)
        got = lax.all_to_all(part, "ep", split_axis=0, concat_axis=0, tiled=True)
        y = expert(got.reshape(-1, model)).reshape(got.shape)
        back = lax.all_to_all(y, "ep", split_axis=0, concat_axis=0, tiled=True)
        back = jnp.swapaxes(back, 0, 1)
        answers = {c: back[..., c * piece : (c + 1) * piece] for c in range(cuts)}

    places = (z * span + jnp.arange(span, dtype=jnp.int32)).astype(F32)
    frequency = ROPE_BASE ** (-jnp.arange(half, dtype=F32) / half)
    angles = places[:, None] * jnp.tile(frequency, width // half)[None, :]
    local_out, lift, packed = call(
        functools.partial(local_kernel, heads),
        (
            jax.ShapeDtypeStruct((span, heads * dv), F32),
            jax.ShapeDtypeStruct((span, width), BF16),
            jax.ShapeDtypeStruct((width + 16, dv), BF16),
        ),
        2_000_000_000, 2_000_000,
        queries, keys, values, log_decay.T, angles,
    )
    state_in = jnp.zeros((width, dv), F32)
    since = jnp.zeros((width,), F32)
    if direct:
        earlier = [
            lax.ppermute(packed, "ep", [(i, i + s) for i in range(ep_n - s)])
            for s in range(1, ep_n)
        ]
    else:
        every = lax.all_gather(packed, "ep")
        earlier = [
            jnp.where(
                z >= s, lax.dynamic_index_in_dim(every, jnp.maximum(z - s, 0), 0, False), 0
            ).astype(BF16)
            for s in range(1, ep_n)
        ]
    for got in earlier:
        got = got.astype(F32)
        state_in = state_in + jnp.exp(since)[:, None] * got[:width]
        since = since + (got[width] + got[width + 8])
    mixed = call(
        functools.partial(finish_kernel, heads),
        jax.ShapeDtypeStruct((span, w_out.shape[1]), BF16),
        4_000_000_000, 4_000_000,
        local_out, lift, state_in.astype(BF16), gate, w_out,
    )
    mixed = mixed.reshape(tp_n, span // tp_n, -1)
    mix_parts = {
        j: lax.dynamic_index_in_dim(mixed, t ^ j, 0, False) for j in range(tp_n)
    }
    mixer_out = scatter_rel(mix_parts, "tp").astype(BF16)

    hidden = {}
    for j in order:
        g = jnp.dot(blocks[j], shared_gate, preferred_element_type=F32)
        u = jnp.dot(blocks[j], shared_up, preferred_element_type=F32)
        hidden[j] = (jax.nn.silu(g) * u).astype(BF16)
    outs = []
    for c in range(cuts):
        parts = {}
        for i, j in enumerate(order):
            down = shared_down[:, c * piece : (c + 1) * piece]
            mine = jnp.dot(hidden[j], down, preferred_element_type=F32)
            routed = lax.dot_general(
                weights[j].reshape(ep_n * cap, rows),
                answers[c][i].reshape(ep_n * cap, piece),
                (((0,), (0,)), ((), ())),
                preferred_element_type=F32,
            )
            parts[j] = mine + routed
        outs.append(scatter_rel(parts, "tp").astype(BF16))
    return mixer_out, jnp.concatenate(outs, axis=1)


def solution(mesh):
    in_specs = (
        P(("grp", "ep"), "tp"),
        P(("grp", "ep"), "tp"),
        P(("grp", "ep"), "tp"),
        P(("grp", "ep"), "tp"),
        P(("grp", "ep"), "tp"),
        P("tp", None),
        P(("grp", "ep", "tp"), None),
        P(),
        P(("grp", "ep", "tp"), None),
        P(("grp", "ep", "tp"), None),
        P(("ep", "tp"), None, None),
        P(("ep", "tp"), None, None),
        P(("ep", "tp"), None, None),
        P(None, "tp"),
        P(None, "tp"),
        P("tp", None),
    )
    out_specs = (P(("grp", "ep", "tp"), None), P(("grp", "ep", "tp"), None))
    return jax.shard_map(
        per_device, mesh=mesh, in_specs=in_specs, out_specs=out_specs, check_vma=False
    )
```

```python
import functools

import jax
import jax.numpy as jnp
import numpy as np
from jax import lax
from jax.experimental import pallas as pl
from jax.experimental.pallas import tpu as pltpu
from jax.sharding import PartitionSpec as P

BLOCK = 128
ROPE_BASE = 10000.0
GROUP_EPS = 1e-05
NORM_EPS = 1e-06
DIRECT = 8
F32 = jnp.float32
BF16 = jnp.bfloat16


def swap(x, axis, bit):
    n = lax.axis_size(axis)
    return lax.ppermute(x, axis, [(i, i ^ bit) for i in range(n)])


def bits_of(n):
    assert n & (n - 1) == 0
    return [1 << i for i in range(n.bit_length() - 1)]


def gather_rel(x, axis):
    blocks = {0: x}
    for bit in reversed(bits_of(lax.axis_size(axis))):
        blocks.update({rel ^ bit: swap(blk, axis, bit) for rel, blk in list(blocks.items())})
    return blocks


def scatter_rel(parts, axis):
    parts = dict(parts)
    for bit in bits_of(lax.axis_size(axis)):
        for rel in [r for r in parts if r & bit]:
            got = swap(parts.pop(rel).astype(BF16), axis, bit)
            parts[rel ^ bit] = parts[rel ^ bit].astype(F32) + got.astype(F32)
    return parts[0]


def rope(x, angles, half):
    lanes = x.shape[1]
    row = lax.broadcasted_iota(jnp.int32, (lanes, lanes), 0)
    col = lax.broadcasted_iota(jnp.int32, (lanes, lanes), 1)
    low = (col % (2 * half)) < half
    turn = jnp.where(
        low & (row == col + half), -1.0, jnp.where((~low) & (row == col - half), 1.0, 0.0)
    ).astype(BF16)
    other = jnp.dot(x, turn, preferred_element_type=F32)
    return x.astype(F32) * jnp.cos(angles) + other * jnp.sin(angles)


def local_kernel(
    heads, q_ref, k_ref, v_ref, d_ref, a_ref, out_ref, lift_ref, state_ref, offset=None
):
    span, width = q_ref.shape
    dk = width // heads
    dv = v_ref.shape[1] // heads
    angles = a_ref[...]
    if offset is not None:
        place = offset + lax.broadcasted_iota(jnp.int32, (span, width), 0)
        angles = place.astype(F32) * angles
    q = rope(q_ref[...], angles, dk // 2).astype(BF16)
    k = (rope(k_ref[...], angles, dk // 2) * dk**-0.5).astype(BF16)
    row = lax.broadcasted_iota(jnp.int32, (BLOCK, BLOCK), 0)
    col = lax.broadcasted_iota(jnp.int32, (BLOCK, BLOCK), 1)
    lower = row >= col
    tri = lower.astype(F32)
    lane = lax.broadcasted_iota(jnp.int32, (BLOCK, width), 1)
    dlane = lax.broadcasted_iota(jnp.int32, (heads, width), 1)
    drow = lax.broadcasted_iota(jnp.int32, (heads, width), 0)
    spread = (dlane // dk == drow).astype(F32)
    state = [jnp.zeros((width, dv), F32) for _ in range(heads)]
    past = jnp.zeros((1, width), F32)
    for b in range(span // BLOCK):
        rows = pl.ds(b * BLOCK, BLOCK)
        at = slice(b * BLOCK, (b + 1) * BLOCK)
        qb, kb = q[at], k[at]
        wide = lax.dot_general(d_ref[:, rows], spread, (((0,), (0,)), ((), ())), precision=lax.Precision.HIGHEST,
                       preferred_element_type=F32)
        run = jnp.dot(tri, wide, precision=lax.Precision.HIGHEST, preferred_element_type=F32)
        last = run[BLOCK - 1 : BLOCK, :]
        lifted = (qb.astype(F32) * jnp.exp(run)).astype(BF16)
        lift_ref[rows, :] = (qb.astype(F32) * jnp.exp(run + past)).astype(BF16)
        tail = (kb.astype(F32) * jnp.exp(last - run)).astype(BF16)
        run_t = run.T
        for h in range(heads):
            mine = lane // dk == h
            zero = jnp.zeros((), BF16)
            qh = jnp.where(mine, qb, zero)
            vb = v_ref[rows, h * dv : (h + 1) * dv]
            scores = lax.dot_general(qh, kb, (((1,), (1,)), ((), ())), preferred_element_type=F32)
            gap = run[:, h * dk : h * dk + 1] - run_t[h * dk : h * dk + 1, :]
            w = jnp.where(lower, scores * jnp.exp(jnp.where(lower, gap, 0.0)), 0.0).astype(BF16)
            out = jnp.dot(w, vb, preferred_element_type=F32)
            if b:
                lh = jnp.where(mine, lifted, zero)
                out = out + jnp.dot(lh, state[h].astype(BF16), preferred_element_type=F32)
            out_ref[rows, h * dv : (h + 1) * dv] = out
            th = jnp.where(mine, tail, zero)
            grown = lax.dot_general(th, vb, (((0,), (0,)), ((), ())), preferred_element_type=F32)
            state[h] = state[h] * jnp.exp(last[:, h * dk : h * dk + 1]) + grown
        past = past + last
    total = state[0]
    for h in range(1, heads):
        total = total + state[h]
    state_ref[:width, :] = total.astype(BF16)
    hi = past.astype(BF16)
    lo = (past - hi.astype(F32)).astype(BF16)
    pad = 8
    state_ref[width : width + pad, :] = jnp.broadcast_to(hi, (pad, width))
    state_ref[width + pad :, :] = jnp.broadcast_to(lo, (pad, width))


def finish_kernel(heads, out_ref, lift_ref, state_ref, gate_ref, w_ref, mix_ref):
    width = lift_ref.shape[1]
    dk = width // heads
    dv = out_ref.shape[1] // heads
    lane = lax.broadcasted_iota(jnp.int32, (BLOCK, width), 1)

    def one(b, carry):
        rows = pl.ds(pl.multiple_of(b * BLOCK, BLOCK), BLOCK)
        lift = lift_ref[rows, :]
        total = jnp.zeros((BLOCK, w_ref.shape[1]), F32)
        for h in range(heads):
            lh = jnp.where(lane // dk == h, lift, jnp.zeros((), BF16))
            r = out_ref[rows, h * dv : (h + 1) * dv] + jnp.dot(
                lh, state_ref[...], preferred_element_type=F32
            )
            r = r - jnp.mean(r, axis=-1, keepdims=True)
            r = r * lax.rsqrt(jnp.mean(r * r, axis=-1, keepdims=True) + GROUP_EPS)
            g = gate_ref[rows, h * dv : (h + 1) * dv].astype(F32)
            y = (g * jax.nn.sigmoid(g) * r).astype(BF16)
            total = total + jnp.dot(
                y, w_ref[h * dv : (h + 1) * dv, :], preferred_element_type=F32
            )
        mix_ref[rows, :] = total.astype(BF16)
        return carry

    lax.fori_loop(0, out_ref.shape[0] // BLOCK, one, 0)


def call(kernel, out_shape, flops, moved, *args):
    vmem = pl.BlockSpec(memory_space=pltpu.VMEM)
    return pl.pallas_call(
        kernel,
        out_shape=out_shape,
        in_specs=[vmem] * len(args),
        out_specs=jax.tree.map(lambda _: vmem, out_shape),
        cost_estimate=pl.CostEstimate(flops=flops, bytes_accessed=moved, transcendentals=0),
        compiler_params=pltpu.CompilerParams(vmem_limit_bytes=32 << 20),
    )(*args)


def semaphores(cuts, subs):
    sizes = dict(
        meta=3, rows=5, state=3, near=2, fmeta=4, mix=2, mix2=cuts, nback=2 * cuts,
        first=2 * cuts, second=cuts, dense=4 * subs, far=8 * subs, back=16 * subs,
        pass_on=4 * subs, fin=2 * subs, fpass=2 * subs,
    )
    base, total = {}, 0
    for name, size in sizes.items():
        base[name] = total
        total += size
    return base, total


SENDS = 192
PASSED = (0, )
FIRST = 2


class At:
    def __init__(self, ref):
        self.ref = ref

    def __getitem__(self, index):
        return self.ref, index


def mega_kernel(
    dims,
    q_hbm, k_hbm, v_hbm, gate_hbm, d_ref, f_ref, x_hbm, gain_ref, route_ref, weigh_ref,
    wo_hbm, eg_hbm, eu_hbm, ed_hbm, sg_hbm, su_hbm, sd_hbm,
    mix_out, moe_out,
    lout, lift, spack, srecv, nbuf, mbuf, fmeta, fbuf, pfar, afar, yfar, pass_buf, ycomb, dsend, fin, fpass,
    wfar, pfar_pick, stbuf, psendn, parrn, ysendn, yrecv, wbuf, hbuf,
    mpart, mrecv, opart, orecv, wo, eg, eu, ed, sg, su, sd,
    q_ref, k_ref, v_ref, gate_ref, x_ref, send_sem, recv_sem, local_sem,
):
    heads, ep_n, tp_n, cap, top, cuts, subs = dims
    z, t = lax.axis_index("ep"), lax.axis_index("tp")
    rows, model = x_ref.shape
    span, width = q_ref.shape
    piece = model // cuts
    part_w = model // (2 * subs)
    pair = 2 * cap
    half_n = tp_n // 2
    bits = bits_of(tp_n)
    sems, _ = semaphores(cuts, subs)

    core = lax.rem(t, 2)
    cx = [core, 1 - core]
    line = t - core
    tps = [t, line + 1 - core, tp_n - 2 - line + core, tp_n - 1 - t]
    ends = [line, line + 1]
    side = z // 2
    near = z + 1 - 2 * lax.rem(z, 2)
    inner = (z == 1) | (z == 2)
    outer = jnp.logical_not(inner)
    relay = 2 - side
    near_peer = {"ep": near}
    crossing = {"ep": relay}

    barrier = pltpu.get_barrier_semaphore()
    for s in range(ep_n):
        for r in range(tp_n):
            if s or r:
                pl.semaphore_signal(
                    barrier, 1, device_id={"ep": lax.rem(z + s, ep_n), "tp": tps[r]}
                )

    early = []
    for i, (a, b) in enumerate(
        ((x_hbm, x_ref), (q_hbm, q_ref), (k_hbm, k_ref), (v_hbm, v_ref), (gate_hbm, gate_ref))
    ):
        early.append(pltpu.make_async_copy(a, b, local_sem.at[7 + i]))
        early[-1].start()
    loads = []
    for i, (a, b) in enumerate(
        ((sg_hbm, sg), (su_hbm, su), (eg_hbm.at[0], eg), (eu_hbm.at[0], eu),
         (ed_hbm.at[0], ed), (wo_hbm, wo), (sd_hbm, sd))
    ):
        loads.append(pltpu.make_async_copy(a, b, local_sem.at[i]))
        loads[-1].start()
    mbuf[0, :top, :] = route_ref[...].astype(F32)
    mbuf[0, top : 2 * top, :] = weigh_ref[...]
    mbuf[0, 2 * top :, :] = jnp.zeros((8 - 2 * top, rows), F32)

    early[0].wait()
    src = x_ref[...].astype(F32)
    scale = lax.rsqrt(jnp.mean(src * src, axis=-1, keepdims=True) + NORM_EPS)
    nbuf[:rows, :] = (src * scale * gain_ref[...]).astype(BF16)
    for s in range(1, ep_n):
        @pl.when(z < s)
        def _():
            srecv[s] = jnp.zeros(srecv.shape[1:], BF16)
    pl.semaphore_wait(barrier, ep_n * tp_n - 1)

    started = []

    def describe(k, i, src, dst, peer):
        src, dst = (r[0].at[r[1]] if isinstance(r, tuple) else r for r in (src, dst))
        return pltpu.make_async_remote_copy(
            src_ref=src, dst_ref=dst, send_sem=send_sem.at[k], recv_sem=recv_sem.at[i],
            device_id=peer,
        )

    only = []

    def when(here):
        if not only:
            return pl.when(here)
        return lambda body: body() if only[-1] is here else None

    def go(i, src, dst, peer, who=None):
        who = only[-1] if only and who is None else who
        job = (len(started), i, src, dst, peer)
        describe(*job).start()
        started.append((job, who))

    def arrived(i, dst):
        describe(0, i, dst, dst, near_peer).wait_recv()

    def block(rel):
        return pl.ds(rel * rows, rows)

    def send_dense(f, sub, who):
        for ch in range(2):
            cols = pl.ds((ch * subs + sub) * part_w, part_w)
            go(
                dense_sem[f][sub], At(nbuf)[block(0), cols], At(fbuf)[f, sub, own_rows],
                {"ep": relay, "tp": ends[ch]}, who,
            )

    own_rows = pl.ds(pl.multiple_of(core * rows, rows), rows)
    dense_sem = [
        [sems["dense"] + 2 * f * subs + core * subs + sub for sub in range(subs)] for f in range(2)
    ]
    fmeta_sem = [sems["fmeta"] + 2 * f + core for f in range(2)]
    mine = [core * subs + sub for sub in range(subs)]
    fin_sem = [sems["fin"] + m for m in mine]
    cross = [[cx[c] * subs + sub for sub in range(subs)] for c in range(2)]
    one, two = {"tp": tps[1]}, {"tp": tps[2]}

    go(sems["meta"], At(mbuf)[0], At(mbuf)[1], one)
    go(sems["rows"], At(nbuf)[block(0)], At(nbuf)[block(1)], one)
    go(sems["meta"] + 1, At(mbuf)[0], At(mbuf)[2], two)
    halves = [pl.ds(h * (model // 2), model // 2) for h in range(2)]
    for h in range(2):
        go(sems["rows"] + 1 + h, At(nbuf)[block(0), halves[h]], At(nbuf)[block(2), halves[h]], two)
    for f, here in ((0, inner), (1, outer)):
        @pl.when(here)
        def _():
            for ch in range(2):
                go(
                    fmeta_sem[f], At(mbuf)[0], At(fmeta)[f, core],
                    {"ep": relay, "tp": ends[ch]}, here,
                )
            if f == 1:
                for sub in range(FIRST):
                    send_dense(f, sub, here)

    lane = lax.broadcasted_iota(jnp.int32, (rows, rows), 1)
    sub_i = lax.broadcasted_iota(jnp.int32, (rows, rows), 0)
    before = (sub_i < lane).astype(BF16)
    slot_id = lax.broadcasted_iota(jnp.int32, (cap, rows), 0).astype(F32)
    blank = jnp.zeros((cap, rows), F32)
    index = lax.broadcasted_iota(jnp.int32, (8, rows), 0)

    def plan(metas, experts):
        names = jnp.full((8, rows), -1, jnp.int32)
        for i, e in enumerate(experts):
            names = jnp.where(index == i, e, names)
        names = names.astype(F32)
        ranks, weights = [], []
        for m in metas:
            hit = [m[k : k + 1, :] == names for k in range(top)]
            mark = functools.reduce(jnp.logical_or, hit)
            weights.append(
                sum(jnp.where(hit[k], m[top + k : top + k + 1, :], 0.0) for k in range(top))
            )
            rank = jnp.dot(
                mark.astype(F32).astype(BF16), before, preferred_element_type=F32
            )
            ranks.append(jnp.where(mark, rank, -1.0))
        picks, scaled = [], []
        for i in range(len(experts)):
            for s in range(2):
                at = jnp.where(slot_id == ranks[s][i : i + 1, :], 1.0, 0.0)
                heavy = at * weights[s][i : i + 1, :]
                picks.append(jnp.concatenate([blank, at] if s else [at, blank], axis=1))
                scaled.append(jnp.concatenate([blank, heavy] if s else [heavy, blank], axis=1))
        return (
            jnp.concatenate(picks, axis=0).astype(BF16),
            jnp.concatenate(scaled, axis=0).astype(BF16),
        )

    def route(g):
        pick, scaled = plan(
            [mbuf[2 * g], mbuf[2 * g + 1]], [z * tp_n + t, near * tp_n + t]
        )
        wbuf[g] = scaled
        sent = jnp.dot(
            pick, nbuf[2 * g * rows : (2 * g + 2) * rows, :], preferred_element_type=F32
        ).astype(BF16)
        psendn[g] = sent[pair:]
        parrn[0, g] = sent[:pair]
        go(sems["near"] + g, At(psendn)[g], At(parrn)[1, g], near_peer)

    def first_rows():
        arrived(sems["meta"], At(mbuf)[1])
        arrived(sems["rows"], At(nbuf)[block(1)])
        route(0)

    def alone(here, step, *args):
        @pl.when(here)
        def _():
            only.append(here)
            step(*args)
            only.pop()

    def early_dense(sub):
        @when(inner)
        def _():
            send_dense(0, sub, inner)

    def late_dense(sub):
        @when(outer)
        def _():
            send_dense(1, sub, outer)

    def local():
        for load in early[1:]:
            load.wait()
        local_kernel(heads, q_ref, k_ref, v_ref, d_ref, f_ref, lout, lift, spack, z * span)

    def states():
        for s in range(1, ep_n):
            later = z + s < ep_n
            after = {"ep": lax.rem(z + s, ep_n)}

            @pl.when(later)
            def _():
                go(sems["state"] + s - 1, spack, At(srecv)[s], after, later)

    def shared(j):
        if j == 0:
            loads[0].wait()
            loads[1].wait()
        x = nbuf[block(j), :]
        g = jnp.dot(x, sg[...], preferred_element_type=F32)
        u = jnp.dot(x, su[...], preferred_element_type=F32)
        hbuf[block(j), :] = (g * jax.nn.sigmoid(g) * u).astype(BF16)

    def gather_states():
        for s in range(1, ep_n):
            @pl.when(z >= s)
            def _():
                arrived(sems["state"] + s - 1, At(srecv)[s])
        state_in = jnp.zeros((width, width), F32)
        since = jnp.zeros((8, width), F32)
        for s in range(1, ep_n):
            got = srecv[s].astype(F32)
            state_in = state_in + jnp.exp(since).T[:, :1] * got[:width]
            since = since + (got[width : width + 8] + got[width + 8 :])
        stbuf[...] = state_in.astype(BF16)
        loads[5].wait()

    def peer_of(j):
        peer = t
        for bit in bits:
            on = lax.rem(j // bit, 2)
            peer = peer + on * (bit - 2 * bit * lax.rem(t // bit, 2))
        return peer

    def finish(first):
        def one_block(i, c):
            j = 2 * i + first
            own = pl.multiple_of(peer_of(j) * (span // tp_n), BLOCK)
            finish_rows(
                heads, lout, lift, stbuf[...], gate_ref, wo, pl.ds(own, span // tp_n), mpart, j
            )
            return c

        lax.fori_loop(0, half_n, one_block, 0)
        if first:
            for i in range(half_n):
                go(sems["mix"] + i, At(mpart)[2 * i + 1], At(mrecv)[i], one)

    def second_rows(h):
        if h == 0:
            arrived(sems["meta"] + 1, At(mbuf)[2])
            go(sems["meta"] + 2, At(mbuf)[2], At(mbuf)[3], one)
        arrived(sems["rows"] + 1 + h, At(nbuf)[block(2), halves[h]])
        go(sems["rows"] + 3 + h, At(nbuf)[block(2), halves[h]], At(nbuf)[block(3), halves[h]], one)

    def mix_add():
        for i in reversed(range(half_n)):
            arrived(sems["mix"] + i, At(mrecv)[i])
            mpart[2 * i] = (mpart[2 * i].astype(F32) + mrecv[i].astype(F32)).astype(BF16)

    def mix_piece(c, who=None):
        cols = pl.ds(c * piece, piece)
        go(sems["mix2"] + c, At(mpart)[2, :, cols], At(mrecv)[half_n, :, cols], two, who)

    def mix_inner(c):
        when(inner)(lambda: mix_piece(c, inner))

    def mix_outer(c):
        when(outer)(lambda: mix_piece(c, outer))

    def mix_done():
        for c in range(cuts):
            arrived(sems["mix2"] + c, At(mrecv)[half_n, :, pl.ds(c * piece, piece)])
        mix_out[...] = (mpart[0].astype(F32) + mrecv[half_n].astype(F32)).astype(BF16)

    def third_rows():
        arrived(sems["meta"] + 2, At(mbuf)[3])
        for h in range(2):
            arrived(sems["rows"] + 3 + h, At(nbuf)[block(3), halves[h]])
        route(1)

    everyone = [
        (near if i // tp_n else z) * tp_n + tps[i % tp_n] for i in range(2 * tp_n)
    ]

    def plan_far(f):
        @when(inner)
        def _():
            for s in range(2):
                arrived(sems["fmeta"] + 2 * f + s, At(fmeta)[f, s])
            pick, scaled = plan([fmeta[f, 0], fmeta[f, 1]], everyone)
            wfar[f] = scaled
            pfar_pick[f] = pick

    def relay_far(f, sub):
        @when(inner)
        def _():
            for s in range(2):
                arrived(sems["dense"] + (2 * f + s) * subs + sub, At(fbuf)[f, sub, block(s)])
            pfar[f, sub] = jnp.dot(
                pfar_pick[f], fbuf[f, sub], preferred_element_type=F32
            ).astype(BF16)
            for i in (6, 7, 4, 5, 2, 3, 1):
                rel = i % tp_n
                go(
                    sems["far"] + (f * subs + sub) * tp_n + rel,
                    At(pfar)[f, sub, pl.ds(i * pair, pair)],
                    At(afar)[f, mine[sub], pl.ds((rel // 2) * pair, pair)],
                    {"ep": near if i // tp_n else z, "tp": tps[rel]}, inner,
                )
            afar[f, mine[sub], :pair] = pfar[f, sub, :pair]

    def hidden(x):
        g = jnp.dot(x, eg[...], preferred_element_type=F32)
        u = jnp.dot(x, eu[...], preferred_element_type=F32)
        return (g * jax.nn.sigmoid(g) * u).astype(BF16)

    def weights():
        for i in (2, 3, 4):
            loads[i].wait()

    def experts_near():
        for g in range(2):
            arrived(sems["near"] + g, At(parrn)[1, g])
        h = hidden(jnp.concatenate([parrn[s, g] for s in range(2) for g in range(2)], axis=0))
        for c in range(cuts):
            at = slice(c * piece, (c + 1) * piece)
            cols = pl.ds(c * piece, piece)
            y = jnp.dot(h, ed[:, at], preferred_element_type=F32).astype(BF16)
            ysendn[:, at] = y[2 * pair :]
            for g in range(2):
                yrecv[g, :pair, at] = y[g * pair : (g + 1) * pair]
                go(
                    sems["nback"] + 2 * c + g, At(ysendn)[pl.ds(g * pair, pair), cols],
                    At(yrecv)[g, pl.ds(pair, pair), cols], near_peer,
                )

    def experts_far(f):
        for sub in range(subs):
            for rel in range(tp_n):
                i = sems["far"] + (f * subs + sub) * tp_n + rel
                dst = At(afar)[f, cross[rel % 2][sub], pl.ds((rel // 2) * pair, pair)]
                if rel:
                    arrived(i, dst)
                else:
                    @when(outer)
                    def _():
                        arrived(i, dst)
        h = hidden(jnp.concatenate([afar[f, q] for q in range(2 * subs)], axis=1))
        for sub in range(subs):
            for ch in range(2):
                q = ch * subs + sub
                yfar[f, q] = jnp.dot(
                    h, ed[:, q * part_w : (q + 1) * part_w], preferred_element_type=F32
                ).astype(BF16)
            base = sems["back"] + (f * subs + sub) * 2 * tp_n

            @when(inner)
            def _():
                for rel in (2, 3, 1):
                    go(
                        base + rel,
                        At(yfar)[f, cross[rel % 2][sub], pl.ds((rel // 2) * pair, pair)],
                        At(ycomb)[f, sub, pl.ds(rel * pair, pair)], {"tp": tps[rel]}, inner,
                    )
                ycomb[f, sub, :pair] = yfar[f, mine[sub], :pair]

            @when(outer)
            def _():
                if f in PASSED:
                    for ch in range(2):
                        q = ch * subs + sub
                        go(
                            sems["pass_on"] + f * 2 * subs + q,
                            At(yfar)[f, q, pl.ds(pair, pair)], At(pass_buf)[f, q], two, outer,
                        )
                for rel in (0, 1) if f in PASSED else (2, 3, 0, 1):
                    go(
                        base + tp_n + rel,
                        At(yfar)[f, cross[rel % 2][sub], pl.ds((rel // 2) * pair, pair)],
                        At(ycomb)[f, sub, pl.ds((tp_n + rel) * pair, pair)],
                        {"ep": near, "tp": tps[rel]}, outer,
                    )

    def pass_far(f, sub):
        @when(outer)
        def _():
            for ch in range(2):
                q = ch * subs + sub
                arrived(sems["pass_on"] + f * 2 * subs + q, At(pass_buf)[f, q])
            for c in range(2):
                go(
                    sems["back"] + (f * subs + sub) * 2 * tp_n + tp_n + 2 + c,
                    At(pass_buf)[f, cross[c][sub]],
                    At(ycomb)[f, sub, pl.ds((tp_n + 2 + c) * pair, pair)],
                    {"ep": near, "tp": tps[c]}, outer,
                )

    def combine_far(f, sub):
        @when(inner)
        def _():
            for i in range(1, 2 * tp_n):
                arrived(
                    sems["back"] + (f * subs + sub) * 2 * tp_n + i,
                    At(ycomb)[f, sub, pl.ds(i * pair, pair)],
                )
            dsend[f, sub] = lax.dot_general(
                wfar[f], ycomb[f, sub], (((0,), (0,)), ((), ())), preferred_element_type=F32
            ).astype(BF16)
            for s in range(2):
                if f:
                    go(
                        sems["fpass"] + 2 * sub + s, At(dsend)[f, sub, block(s)],
                        At(fpass)[sub, block(s)], crossing, inner,
                    )
                else:
                    go(
                        fin_sem[sub], At(dsend)[f, sub, block(s)], At(fin)[mine[sub]],
                        {"ep": relay, "tp": ends[s]}, inner,
                    )

    def pass_fin(sub):
        @when(inner)
        def _():
            for s in range(2):
                arrived(sems["fpass"] + 2 * sub + s, At(fpass)[sub, block(s)])
                go(
                    fin_sem[sub], At(fpass)[sub, block(s)], At(fin)[mine[sub]],
                    {"ep": near, "tp": ends[s]}, inner,
                )

    def combine_near(c):
        if c == 0:
            loads[6].wait()
        at = slice(c * piece, (c + 1) * piece)
        cols = pl.ds(c * piece, piece)
        for g in range(2):
            arrived(sems["nback"] + 2 * c + g, At(yrecv)[g, pl.ds(pair, pair), cols])
        for g in (1, 0):
            part = lax.dot_general(
                wbuf[g], yrecv[g, :, at], (((0,), (0,)), ((), ())), preferred_element_type=F32
            )
            part = part + jnp.dot(
                hbuf[2 * g * rows : (2 * g + 2) * rows, :], sd[:, at], preferred_element_type=F32
            )
            opart[2 * g + 1, :, at] = part[rows:].astype(BF16)
            go(
                sems["first"] + 2 * c + g, At(opart)[2 * g + 1, :, cols],
                At(orecv)[g, :, cols], one,
            )
            opart[2 * g, :, at] = part[:rows].astype(BF16)

    def second(c):
        at = slice(c * piece, (c + 1) * piece)
        cols = pl.ds(c * piece, piece)
        for g in (1, 0):
            arrived(sems["first"] + 2 * c + g, At(orecv)[g, :, cols])
            opart[2 * g, :, at] = (
                opart[2 * g, :, at].astype(F32) + orecv[g, :, at].astype(F32)
            ).astype(BF16)
            if g:
                go(sems["second"] + c, At(opart)[2, :, cols], At(orecv)[2, :, cols], two)

    def moe_done():
        for c in range(cuts):
            arrived(sems["second"] + c, At(orecv)[2, :, pl.ds(c * piece, piece)])
        for sub in range(subs):
            for ch in range(2):
                q = ch * subs + sub
                at = slice(q * part_w, (q + 1) * part_w)
                arrived(sems["fin"] + q, At(fin)[q])
                moe_out[:, at] = (
                    opart[0, :, at].astype(F32) + orecv[2, :, at].astype(F32)
                    + fin[q].astype(F32)
                ).astype(BF16)

    local()
    states()
    early_dense(0)
    early_dense(1)
    first_rows()
    plan_far(1)
    shared(0)
    shared(1)
    relay_far(1, 0)
    second_rows(0)
    relay_far(1, 1)
    second_rows(1)
    third_rows()
    plan_far(0)
    gather_states()
    finish(1)
    finish(0)
    mix_add()
    relay_far(0, 0)
    weights()
    experts_far(1)
    mix_outer(0)
    mix_outer(1)
    relay_far(0, 1)
    mix_inner(0)
    experts_near()
    mix_outer(2)
    mix_outer(3)
    shared(2)
    shared(3)
    combine_far(1, 0)
    combine_far(1, 1)
    experts_far(0)
    pass_far(0, 0)
    pass_far(0, 1)
    mix_inner(1)
    mix_inner(2)
    mix_inner(3)
    combine_near(0)
    combine_near(1)
    second(0)
    combine_near(2)
    second(1)
    pass_fin(0)
    combine_near(3)
    second(2)
    second(3)
    combine_far(0, 0)
    pass_fin(1)
    combine_far(0, 1)
    mix_done()
    moe_done()

    for job, who in started:
        if who is None:
            describe(*job).wait_send()
    conditions = []
    for _, who in started:
        if who is not None and all(who is not w for w in conditions):
            conditions.append(who)
    for w in conditions:
        @pl.when(w)
        def _():
            for job, who in started:
                if who is w:
                    describe(*job).wait_send()
    assert len(started) <= SENDS


def finish_rows(heads, lout, lift_ref, state, gate_ref, wo, at, mpart, j):
    width = lift_ref.shape[1]
    dk = width // heads
    dv = lout.shape[1] // heads
    lift = lift_ref[at, :]
    lane = lax.broadcasted_iota(jnp.int32, lift.shape, 1)
    ys = []
    for h in range(heads):
        lh = jnp.where(lane // dk == h, lift, jnp.zeros((), BF16))
        r = lout[at, h * dv : (h + 1) * dv] + jnp.dot(lh, state, preferred_element_type=F32)
        r = r - jnp.mean(r, axis=-1, keepdims=True)
        r = r * lax.rsqrt(jnp.mean(r * r, axis=-1, keepdims=True) + GROUP_EPS)
        g = gate_ref[at, h * dv : (h + 1) * dv].astype(F32)
        ys.append((g * jax.nn.sigmoid(g) * r).astype(BF16))
    y = jnp.concatenate(ys, axis=1)
    mpart[j] = jnp.dot(y, wo[...], preferred_element_type=F32).astype(BF16)


def mega(
    queries, keys, values, gate, log_decay, w_out, moe_input, moe_gain, routes, route_weight,
    expert_gate, expert_up, expert_down, shared_gate, shared_up, shared_down,
):
    span, width = queries.shape
    heads = log_decay.shape[1]
    half = width // heads // 2
    rows, model = moe_input.shape
    top = routes.shape[1]
    ep_n, tp_n = lax.axis_size("ep"), lax.axis_size("tp")
    cap = rows * top * 3 // (2 * ep_n * tp_n)
    pair, cuts, subs = 2 * cap, 4, 2
    steps = np.arange(half, dtype=np.float32) / np.float32(half)
    freq = np.power(np.float32(ROPE_BASE), -steps).astype(np.float32)
    freq = jnp.asarray(np.tile(freq, width // half)[None, :])
    vmem = pl.BlockSpec(memory_space=pltpu.VMEM)
    hbm = pl.BlockSpec(memory_space=pl.ANY)
    V = pltpu.VMEM
    half_n = tp_n // 2
    part_w = model // (2 * subs)
    copies = semaphores(cuts, subs)[1]
    return pl.pallas_call(
        functools.partial(mega_kernel, (heads, ep_n, tp_n, cap, top, cuts, subs)),
        out_shape=(V((rows, w_out.shape[1]), BF16), V((rows, model), BF16)),
        in_specs=[hbm] * 4 + [vmem] * 2 + [hbm] + [vmem] * 3 + [hbm] * 7,
        out_specs=(vmem, vmem),
        scratch_shapes=[
            V((span, values.shape[1]), F32), V((span, width), BF16),
            V((width + 16, width), BF16), V((ep_n, width + 16, width), BF16),
            V((tp_n * rows, model), BF16), V((tp_n, 8, rows), F32),
            V((2, 2, 8, rows), F32), V((2, subs, 2 * rows, part_w), BF16),
            V((2, subs, 2 * tp_n * pair, part_w), BF16), V((2, 2 * subs, 2 * pair, part_w), BF16),
            V((2, 2 * subs, 2 * pair, part_w), BF16), V((2, 2 * subs, pair, part_w), BF16),
            V((2, subs, 2 * tp_n * pair, part_w), BF16), V((2, subs, 2 * rows, part_w), BF16),
            V((2 * subs, rows, part_w), BF16), V((subs, 2 * rows, part_w), BF16), V((2, 2 * tp_n * pair, 2 * rows), BF16),
            V((2, 2 * tp_n * pair, 2 * rows), BF16), V((width, width), BF16),
            V((2, pair, model), BF16), V((2, 2, pair, model), BF16),
            V((2 * pair, model), BF16), V((2, 2 * pair, model), BF16),
            V((2, 2 * pair, 2 * rows), BF16), V((tp_n * rows, shared_gate.shape[1]), BF16),
            V((tp_n, span // tp_n, w_out.shape[1]), BF16),
            V((half_n + 1, span // tp_n, w_out.shape[1]), BF16),
            V((tp_n, rows, model), BF16), V((half_n + 1, rows, model), BF16),
            V(w_out.shape, BF16), V(expert_gate.shape[1:], BF16), V(expert_up.shape[1:], BF16),
            V(expert_down.shape[1:], BF16), V(shared_gate.shape, BF16),
            V(shared_up.shape, BF16), V(shared_down.shape, BF16),
            V(queries.shape, BF16), V(keys.shape, BF16), V(values.shape, BF16), V(gate.shape, BF16),
            V(moe_input.shape, BF16),
            pltpu.SemaphoreType.DMA((SENDS,)), pltpu.SemaphoreType.DMA((copies,)),
            pltpu.SemaphoreType.DMA((12,)),
        ],
        compiler_params=pltpu.CompilerParams(
            collective_id=0, has_side_effects=True, vmem_limit_bytes=60 << 20
        ),
    )(
        queries, keys, values, gate, log_decay.T, freq, moe_input, moe_gain[None, :],
        routes.T, route_weight.T,
        w_out, expert_gate, expert_up, expert_down, shared_gate, shared_up, shared_down,
    )


def per_device(
    queries, keys, values, gate, log_decay, w_out, moe_input, moe_gain, routes, route_weight,
    expert_gate, expert_up, expert_down, shared_gate, shared_up, shared_down,
):
    span = queries.shape[0]
    heads = log_decay.shape[1]
    width = queries.shape[1]
    dk = width // heads
    half = dk // 2
    dv = values.shape[1] // heads
    rows, model = moe_input.shape
    top = routes.shape[1]
    ep_n, tp_n = lax.axis_size("ep"), lax.axis_size("tp")
    z, t = lax.axis_index("ep"), lax.axis_index("tp")
    direct = ep_n <= DIRECT and ep_n & (ep_n - 1) == 0
    if ep_n == 4 and tp_n == 4 and dv == width and (rows * top * 3 // (ep_n * tp_n)) % 16 == 0:
        return mega(
            queries, keys, values, gate, log_decay, w_out, moe_input, moe_gain, routes,
            route_weight, expert_gate, expert_up, expert_down, shared_gate, shared_up, shared_down,
        )
    cap = rows * top * 3 // (2 * ep_n * tp_n)

    source = moe_input.astype(F32)
    scale_row = lax.rsqrt(jnp.mean(source * source, axis=-1, keepdims=True) + NORM_EPS)
    normed = (source * scale_row * moe_gain[None, :]).astype(BF16)
    meta = jnp.concatenate([routes.astype(F32).T, route_weight.T], axis=0)
    blocks = gather_rel(normed, "tp")
    metas = gather_rel(meta, "tp")
    order = sorted(blocks)

    step = jnp.arange(ep_n, dtype=jnp.int32)
    peers = (z ^ step) if direct else step
    named = (peers * tp_n + t).astype(F32)
    before = (jnp.arange(rows)[:, None] < jnp.arange(rows)[None, :]).astype(BF16)
    parcels, weights = {}, {}
    for j in order:
        hits = metas[j][:top, None, :] == named[None, :, None]
        mark = jnp.any(hits, axis=0)
        weight = jnp.sum(jnp.where(hits, metas[j][top:, None, :], 0.0), axis=0)
        rank = jnp.dot(mark.astype(BF16), before, preferred_element_type=F32)
        slot = mark[:, None, :] & (rank[:, None, :] == jnp.arange(cap, dtype=F32)[None, :, None])
        pick = slot.astype(BF16).reshape(ep_n * cap, rows)
        weights[j] = jnp.where(slot, weight[:, None, :], 0.0).astype(BF16)
        parcels[j] = jnp.dot(pick, blocks[j], preferred_element_type=F32).astype(BF16).reshape(
            ep_n, cap, model
        )

    half_tp = max(1, tp_n // 2)
    groups = [order[:half_tp], order[half_tp:]] if tp_n > 1 else [order]

    def expert(x):
        g = jnp.dot(x, expert_gate[0], preferred_element_type=F32)
        u = jnp.dot(x, expert_up[0], preferred_element_type=F32)
        h = (jax.nn.silu(g) * u).astype(BF16)
        return jnp.dot(h, expert_down[0], preferred_element_type=F32).astype(BF16)

    cuts = 2
    piece = model // cuts
    answers = {}
    if direct:
        arrived = {}
        for group in groups:
            part = jnp.stack([parcels[j] for j in group], axis=1)
            for s in reversed(range(ep_n)):
                got = swap(part[s], "ep", s) if s else part[0]
                arrived.setdefault(s, []).append(got)
        for s in reversed(range(ep_n)):
            flat = jnp.concatenate(arrived[s], axis=0).reshape(tp_n * cap, model)
            y = expert(flat)
            for c in range(cuts):
                back = y[:, c * piece : (c + 1) * piece]
                answers[c, s] = (swap(back, "ep", s) if s else back).reshape(tp_n, cap, piece)
        answers = {
            c: jnp.stack([answers[c, s] for s in range(ep_n)], axis=1) for c in range(cuts)
        }
    else:
        part = jnp.stack([parcels[j] for j in order], axis=1)
        got = lax.all_to_all(part, "ep", split_axis=0, concat_axis=0, tiled=True)
        y = expert(got.reshape(-1, model)).reshape(got.shape)
        back = lax.all_to_all(y, "ep", split_axis=0, concat_axis=0, tiled=True)
        back = jnp.swapaxes(back, 0, 1)
        answers = {c: back[..., c * piece : (c + 1) * piece] for c in range(cuts)}

    places = (z * span + jnp.arange(span, dtype=jnp.int32)).astype(F32)
    frequency = ROPE_BASE ** (-jnp.arange(half, dtype=F32) / half)
    angles = places[:, None] * jnp.tile(frequency, width // half)[None, :]
    local_out, lift, packed = call(
        functools.partial(local_kernel, heads),
        (
            jax.ShapeDtypeStruct((span, heads * dv), F32),
            jax.ShapeDtypeStruct((span, width), BF16),
            jax.ShapeDtypeStruct((width + 16, dv), BF16),
        ),
        2_000_000_000, 2_000_000,
        queries, keys, values, log_decay.T, angles,
    )
    state_in = jnp.zeros((width, dv), F32)
    since = jnp.zeros((width,), F32)
    if direct:
        earlier = [
            lax.ppermute(packed, "ep", [(i, i + s) for i in range(ep_n - s)])
            for s in range(1, ep_n)
        ]
    else:
        every = lax.all_gather(packed, "ep")
        earlier = [
            jnp.where(
                z >= s, lax.dynamic_index_in_dim(every, jnp.maximum(z - s, 0), 0, False), 0
            ).astype(BF16)
            for s in range(1, ep_n)
        ]
    for got in earlier:
        got = got.astype(F32)
        state_in = state_in + jnp.exp(since)[:, None] * got[:width]
        since = since + (got[width] + got[width + 8])
    mixed = call(
        functools.partial(finish_kernel, heads),
        jax.ShapeDtypeStruct((span, w_out.shape[1]), BF16),
        4_000_000_000, 4_000_000,
        local_out, lift, state_in.astype(BF16), gate, w_out,
    )
    mixed = mixed.reshape(tp_n, span // tp_n, -1)
    mix_parts = {
        j: lax.dynamic_index_in_dim(mixed, t ^ j, 0, False) for j in range(tp_n)
    }
    mixer_out = scatter_rel(mix_parts, "tp").astype(BF16)

    hidden = {}
    for j in order:
        g = jnp.dot(blocks[j], shared_gate, preferred_element_type=F32)
        u = jnp.dot(blocks[j], shared_up, preferred_element_type=F32)
        hidden[j] = (jax.nn.silu(g) * u).astype(BF16)
    outs = []
    for c in range(cuts):
        parts = {}
        for i, j in enumerate(order):
            down = shared_down[:, c * piece : (c + 1) * piece]
            mine = jnp.dot(hidden[j], down, preferred_element_type=F32)
            routed = lax.dot_general(
                weights[j].reshape(ep_n * cap, rows),
                answers[c][i].reshape(ep_n * cap, piece),
                (((0,), (0,)), ((), ())),
                preferred_element_type=F32,
            )
            parts[j] = mine + routed
        outs.append(scatter_rel(parts, "tp").astype(BF16))
    return mixer_out, jnp.concatenate(outs, axis=1)


def solution(mesh):
    in_specs = (
        P(("grp", "ep"), "tp"),
        P(("grp", "ep"), "tp"),
        P(("grp", "ep"), "tp"),
        P(("grp", "ep"), "tp"),
        P(("grp", "ep"), "tp"),
        P("tp", None),
        P(("grp", "ep", "tp"), None),
        P(),
        P(("grp", "ep", "tp"), None),
        P(("grp", "ep", "tp"), None),
        P(("ep", "tp"), None, None),
        P(("ep", "tp"), None, None),
        P(("ep", "tp"), None, None),
        P(None, "tp"),
        P(None, "tp"),
        P("tp", None),
    )
    out_specs = (P(("grp", "ep", "tp"), None), P(("grp", "ep", "tp"), None))
    return jax.shard_map(
        per_device, mesh=mesh, in_specs=in_specs, out_specs=out_specs, check_vma=False
    )
```

```python
import functools

import jax
import jax.numpy as jnp
import numpy as np
from jax import lax
from jax.experimental import pallas as pl
from jax.experimental.pallas import tpu as pltpu
from jax.sharding import PartitionSpec as P

BLOCK = 128
ROPE_BASE = 10000.0
GROUP_EPS = 1e-05
NORM_EPS = 1e-06
DIRECT = 8
F32 = jnp.float32
BF16 = jnp.bfloat16


def swap(x, axis, bit):
    n = lax.axis_size(axis)
    return lax.ppermute(x, axis, [(i, i ^ bit) for i in range(n)])


def bits_of(n):
    assert n & (n - 1) == 0
    return [1 << i for i in range(n.bit_length() - 1)]


def gather_rel(x, axis):
    blocks = {0: x}
    for bit in reversed(bits_of(lax.axis_size(axis))):
        blocks.update({rel ^ bit: swap(blk, axis, bit) for rel, blk in list(blocks.items())})
    return blocks


def scatter_rel(parts, axis):
    parts = dict(parts)
    for bit in bits_of(lax.axis_size(axis)):
        for rel in [r for r in parts if r & bit]:
            got = swap(parts.pop(rel).astype(BF16), axis, bit)
            parts[rel ^ bit] = parts[rel ^ bit].astype(F32) + got.astype(F32)
    return parts[0]


def rope(x, angles, half):
    lanes = x.shape[1]
    row = lax.broadcasted_iota(jnp.int32, (lanes, lanes), 0)
    col = lax.broadcasted_iota(jnp.int32, (lanes, lanes), 1)
    low = (col % (2 * half)) < half
    turn = jnp.where(
        low & (row == col + half), -1.0, jnp.where((~low) & (row == col - half), 1.0, 0.0)
    ).astype(BF16)
    other = jnp.dot(x, turn, preferred_element_type=F32)
    return x.astype(F32) * jnp.cos(angles) + other * jnp.sin(angles)


def local_kernel(
    heads, q_ref, k_ref, v_ref, d_ref, a_ref, out_ref, lift_ref, state_ref, offset=None
):
    span, width = q_ref.shape
    dk = width // heads
    dv = v_ref.shape[1] // heads
    angles = a_ref[...]
    if offset is not None:
        place = offset + lax.broadcasted_iota(jnp.int32, (span, width), 0)
        angles = place.astype(F32) * angles
    q = rope(q_ref[...], angles, dk // 2).astype(BF16)
    k = (rope(k_ref[...], angles, dk // 2) * dk**-0.5).astype(BF16)
    row = lax.broadcasted_iota(jnp.int32, (BLOCK, BLOCK), 0)
    col = lax.broadcasted_iota(jnp.int32, (BLOCK, BLOCK), 1)
    lower = row >= col
    tri = lower.astype(F32)
    lane = lax.broadcasted_iota(jnp.int32, (BLOCK, width), 1)
    dlane = lax.broadcasted_iota(jnp.int32, (heads, width), 1)
    drow = lax.broadcasted_iota(jnp.int32, (heads, width), 0)
    spread = (dlane // dk == drow).astype(F32)
    state = [jnp.zeros((width, dv), F32) for _ in range(heads)]
    past = jnp.zeros((1, width), F32)
    for b in range(span // BLOCK):
        rows = pl.ds(b * BLOCK, BLOCK)
        at = slice(b * BLOCK, (b + 1) * BLOCK)
        qb, kb = q[at], k[at]
        wide = lax.dot_general(d_ref[:, rows], spread, (((0,), (0,)), ((), ())), precision=lax.Precision.HIGHEST,
                       preferred_element_type=F32)
        run = jnp.dot(tri, wide, precision=lax.Precision.HIGHEST, preferred_element_type=F32)
        last = run[BLOCK - 1 : BLOCK, :]
        lifted = (qb.astype(F32) * jnp.exp(run)).astype(BF16)
        lift_ref[rows, :] = (qb.astype(F32) * jnp.exp(run + past)).astype(BF16)
        tail = (kb.astype(F32) * jnp.exp(last - run)).astype(BF16)
        run_t = run.T
        for h in range(heads):
            mine = lane // dk == h
            zero = jnp.zeros((), BF16)
            qh = jnp.where(mine, qb, zero)
            vb = v_ref[rows, h * dv : (h + 1) * dv]
            scores = lax.dot_general(qh, kb, (((1,), (1,)), ((), ())), preferred_element_type=F32)
            gap = run[:, h * dk : h * dk + 1] - run_t[h * dk : h * dk + 1, :]
            w = jnp.where(lower, scores * jnp.exp(jnp.where(lower, gap, 0.0)), 0.0).astype(BF16)
            out = jnp.dot(w, vb, preferred_element_type=F32)
            if b:
                lh = jnp.where(mine, lifted, zero)
                out = out + jnp.dot(lh, state[h].astype(BF16), preferred_element_type=F32)
            out_ref[rows, h * dv : (h + 1) * dv] = out
            th = jnp.where(mine, tail, zero)
            grown = lax.dot_general(th, vb, (((0,), (0,)), ((), ())), preferred_element_type=F32)
            state[h] = state[h] * jnp.exp(last[:, h * dk : h * dk + 1]) + grown
        past = past + last
    total = state[0]
    for h in range(1, heads):
        total = total + state[h]
    state_ref[:width, :] = total.astype(BF16)
    hi = past.astype(BF16)
    lo = (past - hi.astype(F32)).astype(BF16)
    pad = 8
    state_ref[width : width + pad, :] = jnp.broadcast_to(hi, (pad, width))
    state_ref[width + pad :, :] = jnp.broadcast_to(lo, (pad, width))


def finish_kernel(heads, out_ref, lift_ref, state_ref, gate_ref, w_ref, mix_ref):
    width = lift_ref.shape[1]
    dk = width // heads
    dv = out_ref.shape[1] // heads
    lane = lax.broadcasted_iota(jnp.int32, (BLOCK, width), 1)

    def one(b, carry):
        rows = pl.ds(pl.multiple_of(b * BLOCK, BLOCK), BLOCK)
        lift = lift_ref[rows, :]
        total = jnp.zeros((BLOCK, w_ref.shape[1]), F32)
        for h in range(heads):
            lh = jnp.where(lane // dk == h, lift, jnp.zeros((), BF16))
            r = out_ref[rows, h * dv : (h + 1) * dv] + jnp.dot(
                lh, state_ref[...], preferred_element_type=F32
            )
            r = r - jnp.mean(r, axis=-1, keepdims=True)
            r = r * lax.rsqrt(jnp.mean(r * r, axis=-1, keepdims=True) + GROUP_EPS)
            g = gate_ref[rows, h * dv : (h + 1) * dv].astype(F32)
            y = (g * jax.nn.sigmoid(g) * r).astype(BF16)
            total = total + jnp.dot(
                y, w_ref[h * dv : (h + 1) * dv, :], preferred_element_type=F32
            )
        mix_ref[rows, :] = total.astype(BF16)
        return carry

    lax.fori_loop(0, out_ref.shape[0] // BLOCK, one, 0)


def call(kernel, out_shape, flops, moved, *args):
    vmem = pl.BlockSpec(memory_space=pltpu.VMEM)
    return pl.pallas_call(
        kernel,
        out_shape=out_shape,
        in_specs=[vmem] * len(args),
        out_specs=jax.tree.map(lambda _: vmem, out_shape),
        cost_estimate=pl.CostEstimate(flops=flops, bytes_accessed=moved, transcendentals=0),
        compiler_params=pltpu.CompilerParams(vmem_limit_bytes=32 << 20),
    )(*args)


def semaphores(cuts, subs):
    sizes = dict(
        meta=3, rows=5, state=3, near=2, fmeta=4, mix=2, mix2=cuts, nback=2 * cuts,
        first=2 * cuts, second=cuts, dense=4 * subs, far=8 * subs, back=16 * subs,
        pass_on=4 * subs, fin=2 * subs, fpass=2 * subs,
    )
    base, total = {}, 0
    for name, size in sizes.items():
        base[name] = total
        total += size
    return base, total


SENDS = 192
PASSED = (0, )
FIRST = 2


class At:
    def __init__(self, ref):
        self.ref = ref

    def __getitem__(self, index):
        return self.ref, index


def mega_kernel(
    dims,
    q_hbm, k_hbm, v_hbm, gate_hbm, d_ref, f_ref, x_hbm, gain_ref, route_ref, weigh_ref,
    wo_hbm, eg_hbm, eu_hbm, ed_hbm, sg_hbm, su_hbm, sd_hbm,
    mix_out, moe_out,
    lout, lift, spack, srecv, nbuf, mbuf, fmeta, fbuf, pfar, afar, yfar, pass_buf, ycomb, dsend, fin, fpass,
    wfar, pfar_pick, stbuf, sumbuf, hnear, psendn, parrn, ysendn, yrecv, wbuf, hbuf,
    mpart, mrecv, opart, orecv, wo, eg, eu, ed, sg, su, sd,
    q_ref, k_ref, v_ref, gate_ref, x_ref, send_sem, recv_sem, local_sem,
):
    heads, ep_n, tp_n, cap, top, cuts, subs = dims
    z, t = lax.axis_index("ep"), lax.axis_index("tp")
    rows, model = x_ref.shape
    span, width = q_ref.shape
    piece = model // cuts
    part_w = model // (2 * subs)
    pair = 2 * cap
    half_n = tp_n // 2
    bits = bits_of(tp_n)
    sems, _ = semaphores(cuts, subs)

    core = lax.rem(t, 2)
    cx = [core, 1 - core]
    line = t - core
    tps = [t, line + 1 - core, tp_n - 2 - line + core, tp_n - 1 - t]
    ends = [line, line + 1]
    side = z // 2
    near = z + 1 - 2 * lax.rem(z, 2)
    inner = (z == 1) | (z == 2)
    outer = jnp.logical_not(inner)
    relay = 2 - side
    near_peer = {"ep": near}
    crossing = {"ep": relay}

    barrier = pltpu.get_barrier_semaphore()
    for s in range(ep_n):
        for r in range(tp_n):
            if s or r:
                pl.semaphore_signal(
                    barrier, 1, device_id={"ep": lax.rem(z + s, ep_n), "tp": tps[r]}
                )

    early = []
    for i, (a, b) in enumerate(
        ((x_hbm, x_ref), (q_hbm, q_ref), (k_hbm, k_ref), (v_hbm, v_ref), (gate_hbm, gate_ref))
    ):
        early.append(pltpu.make_async_copy(a, b, local_sem.at[7 + i]))
        early[-1].start()
    loads = []
    for i, (a, b) in enumerate(
        ((sg_hbm, sg), (su_hbm, su), (eg_hbm.at[0], eg), (eu_hbm.at[0], eu),
         (ed_hbm.at[0], ed), (wo_hbm, wo), (sd_hbm, sd))
    ):
        loads.append(pltpu.make_async_copy(a, b, local_sem.at[i]))
        loads[-1].start()
    mbuf[0, :top, :] = route_ref[...].astype(F32)
    mbuf[0, top : 2 * top, :] = weigh_ref[...]
    mbuf[0, 2 * top :, :] = jnp.zeros((8 - 2 * top, rows), F32)

    early[0].wait()
    src = x_ref[...].astype(F32)
    scale = lax.rsqrt(jnp.mean(src * src, axis=-1, keepdims=True) + NORM_EPS)
    nbuf[:rows, :] = (src * scale * gain_ref[...]).astype(BF16)
    for s in range(1, ep_n):
        @pl.when(z < s)
        def _():
            srecv[s] = jnp.zeros(srecv.shape[1:], BF16)
    pl.semaphore_wait(barrier, ep_n * tp_n - 1)

    started = []

    def describe(k, i, src, dst, peer):
        src, dst = (r[0].at[r[1]] if isinstance(r, tuple) else r for r in (src, dst))
        return pltpu.make_async_remote_copy(
            src_ref=src, dst_ref=dst, send_sem=send_sem.at[k], recv_sem=recv_sem.at[i],
            device_id=peer,
        )

    only = []

    def when(here):
        if not only:
            return pl.when(here)
        return lambda body: body() if only[-1] is here else None

    def go(i, src, dst, peer, who=None):
        who = only[-1] if only and who is None else who
        job = (len(started), i, src, dst, peer)
        describe(*job).start()
        started.append((job, who))

    def arrived(i, dst):
        describe(0, i, dst, dst, near_peer).wait_recv()

    def block(rel):
        return pl.ds(rel * rows, rows)

    def send_dense(f, sub, who):
        for ch in range(2):
            cols = pl.ds((ch * subs + sub) * part_w, part_w)
            go(
                dense_sem[f][sub], At(nbuf)[block(0), cols], At(fbuf)[f, sub, own_rows],
                {"ep": relay, "tp": ends[ch]}, who,
            )

    own_rows = pl.ds(pl.multiple_of(core * rows, rows), rows)
    dense_sem = [
        [sems["dense"] + 2 * f * subs + core * subs + sub for sub in range(subs)] for f in range(2)
    ]
    fmeta_sem = [sems["fmeta"] + 2 * f + core for f in range(2)]
    mine = [core * subs + sub for sub in range(subs)]
    fin_sem = [sems["fin"] + m for m in mine]
    cross = [[cx[c] * subs + sub for sub in range(subs)] for c in range(2)]
    one, two = {"tp": tps[1]}, {"tp": tps[2]}

    go(sems["meta"], At(mbuf)[0], At(mbuf)[1], one)
    go(sems["rows"], At(nbuf)[block(0)], At(nbuf)[block(1)], one)
    go(sems["meta"] + 1, At(mbuf)[0], At(mbuf)[2], two)
    halves = [pl.ds(h * (model // 2), model // 2) for h in range(2)]
    for h in range(2):
        go(sems["rows"] + 1 + h, At(nbuf)[block(0), halves[h]], At(nbuf)[block(2), halves[h]], two)
    for f, here in ((0, inner), (1, outer)):
        @pl.when(here)
        def _():
            for ch in range(2):
                go(
                    fmeta_sem[f], At(mbuf)[0], At(fmeta)[f, core],
                    {"ep": relay, "tp": ends[ch]}, here,
                )
            if f == 1:
                for sub in range(FIRST):
                    send_dense(f, sub, here)

    lane = lax.broadcasted_iota(jnp.int32, (rows, rows), 1)
    sub_i = lax.broadcasted_iota(jnp.int32, (rows, rows), 0)
    before = (sub_i < lane).astype(BF16)
    slot_id = lax.broadcasted_iota(jnp.int32, (cap, rows), 0).astype(F32)
    blank = jnp.zeros((cap, rows), F32)
    index = lax.broadcasted_iota(jnp.int32, (8, rows), 0)

    def plan(metas, experts):
        names = jnp.full((8, rows), -1, jnp.int32)
        for i, e in enumerate(experts):
            names = jnp.where(index == i, e, names)
        names = names.astype(F32)
        ranks, weights = [], []
        for m in metas:
            hit = [m[k : k + 1, :] == names for k in range(top)]
            mark = functools.reduce(jnp.logical_or, hit)
            weights.append(
                sum(jnp.where(hit[k], m[top + k : top + k + 1, :], 0.0) for k in range(top))
            )
            rank = jnp.dot(
                mark.astype(F32).astype(BF16), before, preferred_element_type=F32
            )
            ranks.append(jnp.where(mark, rank, -1.0))
        picks, scaled = [], []
        for i in range(len(experts)):
            for s in range(2):
                at = jnp.where(slot_id == ranks[s][i : i + 1, :], 1.0, 0.0)
                heavy = at * weights[s][i : i + 1, :]
                picks.append(jnp.concatenate([blank, at] if s else [at, blank], axis=1))
                scaled.append(jnp.concatenate([blank, heavy] if s else [heavy, blank], axis=1))
        return (
            jnp.concatenate(picks, axis=0).astype(BF16),
            jnp.concatenate(scaled, axis=0).astype(BF16),
        )

    def route(g):
        pick, scaled = plan(
            [mbuf[2 * g], mbuf[2 * g + 1]], [z * tp_n + t, near * tp_n + t]
        )
        wbuf[g] = scaled
        sent = jnp.dot(
            pick, nbuf[2 * g * rows : (2 * g + 2) * rows, :], preferred_element_type=F32
        ).astype(BF16)
        psendn[g] = sent[pair:]
        parrn[0, g] = sent[:pair]
        go(sems["near"] + g, At(psendn)[g], At(parrn)[1, g], near_peer)

    def first_rows():
        arrived(sems["meta"], At(mbuf)[1])
        arrived(sems["rows"], At(nbuf)[block(1)])
        route(0)

    def alone(here, step, *args):
        @pl.when(here)
        def _():
            only.append(here)
            step(*args)
            only.pop()

    def early_dense(sub):
        @when(inner)
        def _():
            send_dense(0, sub, inner)

    def late_dense(sub):
        @when(outer)
        def _():
            send_dense(1, sub, outer)

    def local():
        for load in early[1:]:
            load.wait()
        local_kernel(heads, q_ref, k_ref, v_ref, d_ref, f_ref, lout, lift, spack, z * span)

    def states():
        for s in range(1, ep_n - 1):
            later = z + s < ep_n - 1
            after = {"ep": lax.rem(z + s, ep_n)}

            @pl.when(later)
            def _():
                go(sems["state"] + s, spack, At(srecv)[s], after, later)

    def shared(j):
        if j == 0:
            loads[0].wait()
            loads[1].wait()
        x = nbuf[block(j), :]
        g = jnp.dot(x, sg[...], preferred_element_type=F32)
        u = jnp.dot(x, su[...], preferred_element_type=F32)
        hbuf[block(j), :] = (g * jax.nn.sigmoid(g) * u).astype(BF16)

    ends_here = z == ep_n - 1
    hands_on = z == ep_n - 2
    next_peer = {"ep": lax.rem(z + 1, ep_n)}

    def gather_states():
        for s in range(1, ep_n - 1):
            @pl.when((z >= s) & (z < ep_n - 1))
            def _():
                arrived(sems["state"] + s, At(srecv)[s])

        @pl.when(ends_here)
        def _():
            arrived(sems["state"], At(srecv)[1, pl.ds(0, width)])

        state_in = jnp.zeros((width, width), F32)
        since = jnp.zeros((8, width), F32)
        for s in range(1, ep_n):
            got = srecv[s].astype(F32)
            state_in = state_in + jnp.exp(since).T[:, :1] * got[:width]
            since = since + (got[width : width + 8] + got[width + 8 :])
        stbuf[...] = state_in.astype(BF16)
        if not only or only[-1] is inner:
            @pl.when(hands_on)
            def _():
                own = spack[...].astype(F32)
                past = own[width : width + 8] + own[width + 8 :]
                total = own[:width] + jnp.exp(past).T[:, :1] * stbuf[...].astype(F32)
                sumbuf[...] = total.astype(BF16)
                go(sems["state"], sumbuf, At(srecv)[1, pl.ds(0, width)], next_peer, hands_on)

        loads[5].wait()

    def peer_of(j):
        peer = t
        for bit in bits:
            on = lax.rem(j // bit, 2)
            peer = peer + on * (bit - 2 * bit * lax.rem(t // bit, 2))
        return peer

    def finish(first):
        def one_block(i, c):
            j = 2 * i + first
            own = pl.multiple_of(peer_of(j) * (span // tp_n), BLOCK)
            finish_rows(
                heads, lout, lift, stbuf[...], gate_ref, wo, pl.ds(own, span // tp_n), mpart, j
            )
            return c

        lax.fori_loop(0, half_n, one_block, 0)
        if first:
            for i in range(half_n):
                go(sems["mix"] + i, At(mpart)[2 * i + 1], At(mrecv)[i], one)

    def second_rows(h):
        if h == 0:
            arrived(sems["meta"] + 1, At(mbuf)[2])
            go(sems["meta"] + 2, At(mbuf)[2], At(mbuf)[3], one)
        arrived(sems["rows"] + 1 + h, At(nbuf)[block(2), halves[h]])
        go(sems["rows"] + 3 + h, At(nbuf)[block(2), halves[h]], At(nbuf)[block(3), halves[h]], one)

    def mix_add():
        for i in reversed(range(half_n)):
            arrived(sems["mix"] + i, At(mrecv)[i])
            mpart[2 * i] = (mpart[2 * i].astype(F32) + mrecv[i].astype(F32)).astype(BF16)

    def mix_piece(c, who=None):
        cols = pl.ds(c * piece, piece)
        go(sems["mix2"] + c, At(mpart)[2, :, cols], At(mrecv)[half_n, :, cols], two, who)

    def mix_inner(c):
        when(inner)(lambda: mix_piece(c, inner))

    def mix_outer(c):
        when(outer)(lambda: mix_piece(c, outer))

    def mix_done():
        for c in range(cuts):
            arrived(sems["mix2"] + c, At(mrecv)[half_n, :, pl.ds(c * piece, piece)])
        mix_out[...] = (mpart[0].astype(F32) + mrecv[half_n].astype(F32)).astype(BF16)

    def third_rows():
        arrived(sems["meta"] + 2, At(mbuf)[3])
        for h in range(2):
            arrived(sems["rows"] + 3 + h, At(nbuf)[block(3), halves[h]])
        route(1)

    everyone = [
        (near if i // tp_n else z) * tp_n + tps[i % tp_n] for i in range(2 * tp_n)
    ]

    def plan_far(f):
        @when(inner)
        def _():
            for s in range(2):
                arrived(sems["fmeta"] + 2 * f + s, At(fmeta)[f, s])
            pick, scaled = plan([fmeta[f, 0], fmeta[f, 1]], everyone)
            wfar[f] = scaled
            pfar_pick[f] = pick

    def relay_far(f, sub):
        @when(inner)
        def _():
            for s in range(2):
                arrived(sems["dense"] + (2 * f + s) * subs + sub, At(fbuf)[f, sub, block(s)])
            pfar[f, sub] = jnp.dot(
                pfar_pick[f], fbuf[f, sub], preferred_element_type=F32
            ).astype(BF16)
            for i in (6, 7, 4, 5, 2, 3, 1):
                rel = i % tp_n
                go(
                    sems["far"] + (f * subs + sub) * tp_n + rel,
                    At(pfar)[f, sub, pl.ds(i * pair, pair)],
                    At(afar)[f, mine[sub], pl.ds((rel // 2) * pair, pair)],
                    {"ep": near if i // tp_n else z, "tp": tps[rel]}, inner,
                )
            afar[f, mine[sub], :pair] = pfar[f, sub, :pair]

    def hidden(x):
        g = jnp.dot(x, eg[...], preferred_element_type=F32)
        u = jnp.dot(x, eu[...], preferred_element_type=F32)
        return (g * jax.nn.sigmoid(g) * u).astype(BF16)

    def weights():
        for i in (2, 3, 4):
            loads[i].wait()

    def near_hidden():
        for g in range(2):
            arrived(sems["near"] + g, At(parrn)[1, g])
        hnear[...] = hidden(
            jnp.concatenate([parrn[s, g] for s in range(2) for g in range(2)], axis=0)
        )

    def near_out(c):
        at = slice(c * piece, (c + 1) * piece)
        cols = pl.ds(c * piece, piece)
        y = jnp.dot(hnear[...], ed[:, at], preferred_element_type=F32).astype(BF16)
        ysendn[:, at] = y[2 * pair :]
        for g in range(2):
            yrecv[g, :pair, at] = y[g * pair : (g + 1) * pair]
            go(
                sems["nback"] + 2 * c + g, At(ysendn)[pl.ds(g * pair, pair), cols],
                At(yrecv)[g, pl.ds(pair, pair), cols], near_peer,
            )

    def experts_far(f):
        for sub in range(subs):
            for rel in range(tp_n):
                i = sems["far"] + (f * subs + sub) * tp_n + rel
                dst = At(afar)[f, cross[rel % 2][sub], pl.ds((rel // 2) * pair, pair)]
                if rel:
                    arrived(i, dst)
                else:
                    @when(outer)
                    def _():
                        arrived(i, dst)
        h = hidden(jnp.concatenate([afar[f, q] for q in range(2 * subs)], axis=1))
        for sub in range(subs):
            for ch in range(2):
                q = ch * subs + sub
                yfar[f, q] = jnp.dot(
                    h, ed[:, q * part_w : (q + 1) * part_w], preferred_element_type=F32
                ).astype(BF16)
            base = sems["back"] + (f * subs + sub) * 2 * tp_n

            @when(inner)
            def _():
                for rel in (2, 3, 1):
                    go(
                        base + rel,
                        At(yfar)[f, cross[rel % 2][sub], pl.ds((rel // 2) * pair, pair)],
                        At(ycomb)[f, sub, pl.ds(rel * pair, pair)], {"tp": tps[rel]}, inner,
                    )
                ycomb[f, sub, :pair] = yfar[f, mine[sub], :pair]

            @when(outer)
            def _():
                if f in PASSED:
                    for ch in range(2):
                        q = ch * subs + sub
                        go(
                            sems["pass_on"] + f * 2 * subs + q,
                            At(yfar)[f, q, pl.ds(pair, pair)], At(pass_buf)[f, q], two, outer,
                        )
                for rel in (0, 1) if f in PASSED else (2, 3, 0, 1):
                    go(
                        base + tp_n + rel,
                        At(yfar)[f, cross[rel % 2][sub], pl.ds((rel // 2) * pair, pair)],
                        At(ycomb)[f, sub, pl.ds((tp_n + rel) * pair, pair)],
                        {"ep": near, "tp": tps[rel]}, outer,
                    )

    def pass_far(f, sub):
        @when(outer)
        def _():
            for ch in range(2):
                q = ch * subs + sub
                arrived(sems["pass_on"] + f * 2 * subs + q, At(pass_buf)[f, q])
            for c in range(2):
                go(
                    sems["back"] + (f * subs + sub) * 2 * tp_n + tp_n + 2 + c,
                    At(pass_buf)[f, cross[c][sub]],
                    At(ycomb)[f, sub, pl.ds((tp_n + 2 + c) * pair, pair)],
                    {"ep": near, "tp": tps[c]}, outer,
                )

    def combine_far(f, sub):
        @when(inner)
        def _():
            for i in range(1, 2 * tp_n):
                arrived(
                    sems["back"] + (f * subs + sub) * 2 * tp_n + i,
                    At(ycomb)[f, sub, pl.ds(i * pair, pair)],
                )
            dsend[f, sub] = lax.dot_general(
                wfar[f], ycomb[f, sub], (((0,), (0,)), ((), ())), preferred_element_type=F32
            ).astype(BF16)
            for s in range(2):
                if f:
                    go(
                        sems["fpass"] + 2 * sub + s, At(dsend)[f, sub, block(s)],
                        At(fpass)[sub, block(s)], crossing, inner,
                    )
                else:
                    go(
                        fin_sem[sub], At(dsend)[f, sub, block(s)], At(fin)[mine[sub]],
                        {"ep": relay, "tp": ends[s]}, inner,
                    )

    def pass_fin(sub):
        @when(inner)
        def _():
            for s in range(2):
                arrived(sems["fpass"] + 2 * sub + s, At(fpass)[sub, block(s)])
                go(
                    fin_sem[sub], At(fpass)[sub, block(s)], At(fin)[mine[sub]],
                    {"ep": near, "tp": ends[s]}, inner,
                )

    def combine_near(c):
        if c == 0:
            loads[6].wait()
        at = slice(c * piece, (c + 1) * piece)
        cols = pl.ds(c * piece, piece)
        for g in range(2):
            arrived(sems["nback"] + 2 * c + g, At(yrecv)[g, pl.ds(pair, pair), cols])
        for g in (1, 0):
            part = lax.dot_general(
                wbuf[g], yrecv[g, :, at], (((0,), (0,)), ((), ())), preferred_element_type=F32
            )
            part = part + jnp.dot(
                hbuf[2 * g * rows : (2 * g + 2) * rows, :], sd[:, at], preferred_element_type=F32
            )
            opart[2 * g + 1, :, at] = part[rows:].astype(BF16)
            go(
                sems["first"] + 2 * c + g, At(opart)[2 * g + 1, :, cols],
                At(orecv)[g, :, cols], one,
            )
            opart[2 * g, :, at] = part[:rows].astype(BF16)

    def second(c):
        at = slice(c * piece, (c + 1) * piece)
        cols = pl.ds(c * piece, piece)
        for g in (1, 0):
            arrived(sems["first"] + 2 * c + g, At(orecv)[g, :, cols])
            opart[2 * g, :, at] = (
                opart[2 * g, :, at].astype(F32) + orecv[g, :, at].astype(F32)
            ).astype(BF16)
            if g:
                go(sems["second"] + c, At(opart)[2, :, cols], At(orecv)[2, :, cols], two)

    def moe_done():
        for c in range(cuts):
            arrived(sems["second"] + c, At(orecv)[2, :, pl.ds(c * piece, piece)])
        for sub in range(subs):
            for ch in range(2):
                q = ch * subs + sub
                at = slice(q * part_w, (q + 1) * part_w)
                arrived(sems["fin"] + q, At(fin)[q])
                moe_out[:, at] = (
                    opart[0, :, at].astype(F32) + orecv[2, :, at].astype(F32)
                    + fin[q].astype(F32)
                ).astype(BF16)

    local()
    states()
    early_dense(0)
    early_dense(1)
    first_rows()
    plan_far(1)
    shared(0)
    shared(1)
    relay_far(1, 0)
    second_rows(0)
    relay_far(1, 1)
    second_rows(1)
    third_rows()
    plan_far(0)
    alone(inner, gather_states)
    alone(inner, finish, 1)
    alone(inner, finish, 0)
    alone(inner, mix_add)
    relay_far(0, 0)
    weights()
    experts_far(1)
    alone(outer, near_hidden)
    alone(outer, near_out, 0)
    alone(outer, near_out, 1)
    alone(outer, near_out, 2)
    alone(outer, near_out, 3)
    alone(outer, gather_states)
    alone(outer, finish, 1)
    alone(outer, finish, 0)
    alone(outer, mix_add)
    mix_outer(0)
    mix_outer(1)
    alone(outer, shared, 2)
    alone(outer, shared, 3)
    alone(outer, experts_far, 0)
    mix_outer(2)
    mix_outer(3)
    pass_far(0, 0)
    pass_far(0, 1)
    relay_far(0, 1)
    mix_inner(0)
    alone(inner, near_hidden)
    alone(inner, near_out, 0)
    alone(inner, near_out, 1)
    alone(inner, near_out, 2)
    alone(inner, near_out, 3)
    alone(inner, shared, 2)
    alone(inner, shared, 3)
    combine_far(1, 0)
    combine_far(1, 1)
    alone(inner, experts_far, 0)
    mix_inner(1)
    mix_inner(2)
    mix_inner(3)
    combine_near(0)
    combine_near(1)
    second(0)
    second(1)
    pass_fin(0)
    combine_far(0, 0)
    combine_far(0, 1)
    pass_fin(1)
    combine_near(2)
    combine_near(3)
    second(2)
    second(3)
    mix_done()
    moe_done()

    for job, who in started:
        if who is None:
            describe(*job).wait_send()
    conditions = []
    for _, who in started:
        if who is not None and all(who is not w for w in conditions):
            conditions.append(who)
    for w in conditions:
        @pl.when(w)
        def _():
            for job, who in started:
                if who is w:
                    describe(*job).wait_send()
    assert len(started) <= SENDS


def finish_rows(heads, lout, lift_ref, state, gate_ref, wo, at, mpart, j):
    width = lift_ref.shape[1]
    dk = width // heads
    dv = lout.shape[1] // heads
    lift = lift_ref[at, :]
    lane = lax.broadcasted_iota(jnp.int32, lift.shape, 1)
    ys = []
    for h in range(heads):
        lh = jnp.where(lane // dk == h, lift, jnp.zeros((), BF16))
        r = lout[at, h * dv : (h + 1) * dv] + jnp.dot(lh, state, preferred_element_type=F32)
        r = r - jnp.mean(r, axis=-1, keepdims=True)
        r = r * lax.rsqrt(jnp.mean(r * r, axis=-1, keepdims=True) + GROUP_EPS)
        g = gate_ref[at, h * dv : (h + 1) * dv].astype(F32)
        ys.append((g * jax.nn.sigmoid(g) * r).astype(BF16))
    y = jnp.concatenate(ys, axis=1)
    mpart[j] = jnp.dot(y, wo[...], preferred_element_type=F32).astype(BF16)


def mega(
    queries, keys, values, gate, log_decay, w_out, moe_input, moe_gain, routes, route_weight,
    expert_gate, expert_up, expert_down, shared_gate, shared_up, shared_down,
):
    span, width = queries.shape
    heads = log_decay.shape[1]
    half = width // heads // 2
    rows, model = moe_input.shape
    top = routes.shape[1]
    ep_n, tp_n = lax.axis_size("ep"), lax.axis_size("tp")
    cap = rows * top * 3 // (2 * ep_n * tp_n)
    pair, cuts, subs = 2 * cap, 4, 2
    steps = np.arange(half, dtype=np.float32) / np.float32(half)
    freq = np.power(np.float32(ROPE_BASE), -steps).astype(np.float32)
    freq = jnp.asarray(np.tile(freq, width // half)[None, :])
    vmem = pl.BlockSpec(memory_space=pltpu.VMEM)
    hbm = pl.BlockSpec(memory_space=pl.ANY)
    V = pltpu.VMEM
    half_n = tp_n // 2
    part_w = model // (2 * subs)
    copies = semaphores(cuts, subs)[1]
    return pl.pallas_call(
        functools.partial(mega_kernel, (heads, ep_n, tp_n, cap, top, cuts, subs)),
        out_shape=(V((rows, w_out.shape[1]), BF16), V((rows, model), BF16)),
        in_specs=[hbm] * 4 + [vmem] * 2 + [hbm] + [vmem] * 3 + [hbm] * 7,
        out_specs=(vmem, vmem),
        scratch_shapes=[
            V((span, values.shape[1]), F32), V((span, width), BF16),
            V((width + 16, width), BF16), V((ep_n, width + 16, width), BF16),
            V((tp_n * rows, model), BF16), V((tp_n, 8, rows), F32),
            V((2, 2, 8, rows), F32), V((2, subs, 2 * rows, part_w), BF16),
            V((2, subs, 2 * tp_n * pair, part_w), BF16), V((2, 2 * subs, 2 * pair, part_w), BF16),
            V((2, 2 * subs, 2 * pair, part_w), BF16), V((2, 2 * subs, pair, part_w), BF16),
            V((2, subs, 2 * tp_n * pair, part_w), BF16), V((2, subs, 2 * rows, part_w), BF16),
            V((2 * subs, rows, part_w), BF16), V((subs, 2 * rows, part_w), BF16), V((2, 2 * tp_n * pair, 2 * rows), BF16),
            V((2, 2 * tp_n * pair, 2 * rows), BF16), V((width, width), BF16), V((width, width), BF16),
            V((4 * pair, expert_gate.shape[2]), BF16),
            V((2, pair, model), BF16), V((2, 2, pair, model), BF16),
            V((2 * pair, model), BF16), V((2, 2 * pair, model), BF16),
            V((2, 2 * pair, 2 * rows), BF16), V((tp_n * rows, shared_gate.shape[1]), BF16),
            V((tp_n, span // tp_n, w_out.shape[1]), BF16),
            V((half_n + 1, span // tp_n, w_out.shape[1]), BF16),
            V((tp_n, rows, model), BF16), V((half_n + 1, rows, model), BF16),
            V(w_out.shape, BF16), V(expert_gate.shape[1:], BF16), V(expert_up.shape[1:], BF16),
            V(expert_down.shape[1:], BF16), V(shared_gate.shape, BF16),
            V(shared_up.shape, BF16), V(shared_down.shape, BF16),
            V(queries.shape, BF16), V(keys.shape, BF16), V(values.shape, BF16), V(gate.shape, BF16),
            V(moe_input.shape, BF16),
            pltpu.SemaphoreType.DMA((SENDS,)), pltpu.SemaphoreType.DMA((copies,)),
            pltpu.SemaphoreType.DMA((12,)),
        ],
        compiler_params=pltpu.CompilerParams(
            collective_id=0, has_side_effects=True, vmem_limit_bytes=60 << 20
        ),
    )(
        queries, keys, values, gate, log_decay.T, freq, moe_input, moe_gain[None, :],
        routes.T, route_weight.T,
        w_out, expert_gate, expert_up, expert_down, shared_gate, shared_up, shared_down,
    )


def per_device(
    queries, keys, values, gate, log_decay, w_out, moe_input, moe_gain, routes, route_weight,
    expert_gate, expert_up, expert_down, shared_gate, shared_up, shared_down,
):
    span = queries.shape[0]
    heads = log_decay.shape[1]
    width = queries.shape[1]
    dk = width // heads
    half = dk // 2
    dv = values.shape[1] // heads
    rows, model = moe_input.shape
    top = routes.shape[1]
    ep_n, tp_n = lax.axis_size("ep"), lax.axis_size("tp")
    z, t = lax.axis_index("ep"), lax.axis_index("tp")
    direct = ep_n <= DIRECT and ep_n & (ep_n - 1) == 0
    if ep_n == 4 and tp_n == 4 and dv == width and (rows * top * 3 // (ep_n * tp_n)) % 16 == 0:
        return mega(
            queries, keys, values, gate, log_decay, w_out, moe_input, moe_gain, routes,
            route_weight, expert_gate, expert_up, expert_down, shared_gate, shared_up, shared_down,
        )
    cap = rows * top * 3 // (2 * ep_n * tp_n)

    source = moe_input.astype(F32)
    scale_row = lax.rsqrt(jnp.mean(source * source, axis=-1, keepdims=True) + NORM_EPS)
    normed = (source * scale_row * moe_gain[None, :]).astype(BF16)
    meta = jnp.concatenate([routes.astype(F32).T, route_weight.T], axis=0)
    blocks = gather_rel(normed, "tp")
    metas = gather_rel(meta, "tp")
    order = sorted(blocks)

    step = jnp.arange(ep_n, dtype=jnp.int32)
    peers = (z ^ step) if direct else step
    named = (peers * tp_n + t).astype(F32)
    before = (jnp.arange(rows)[:, None] < jnp.arange(rows)[None, :]).astype(BF16)
    parcels, weights = {}, {}
    for j in order:
        hits = metas[j][:top, None, :] == named[None, :, None]
        mark = jnp.any(hits, axis=0)
        weight = jnp.sum(jnp.where(hits, metas[j][top:, None, :], 0.0), axis=0)
        rank = jnp.dot(mark.astype(BF16), before, preferred_element_type=F32)
        slot = mark[:, None, :] & (rank[:, None, :] == jnp.arange(cap, dtype=F32)[None, :, None])
        pick = slot.astype(BF16).reshape(ep_n * cap, rows)
        weights[j] = jnp.where(slot, weight[:, None, :], 0.0).astype(BF16)
        parcels[j] = jnp.dot(pick, blocks[j], preferred_element_type=F32).astype(BF16).reshape(
            ep_n, cap, model
        )

    half_tp = max(1, tp_n // 2)
    groups = [order[:half_tp], order[half_tp:]] if tp_n > 1 else [order]

    def expert(x):
        g = jnp.dot(x, expert_gate[0], preferred_element_type=F32)
        u = jnp.dot(x, expert_up[0], preferred_element_type=F32)
        h = (jax.nn.silu(g) * u).astype(BF16)
        return jnp.dot(h, expert_down[0], preferred_element_type=F32).astype(BF16)

    cuts = 2
    piece = model // cuts
    answers = {}
    if direct:
        arrived = {}
        for group in groups:
            part = jnp.stack([parcels[j] for j in group], axis=1)
            for s in reversed(range(ep_n)):
                got = swap(part[s], "ep", s) if s else part[0]
                arrived.setdefault(s, []).append(got)
        for s in reversed(range(ep_n)):
            flat = jnp.concatenate(arrived[s], axis=0).reshape(tp_n * cap, model)
            y = expert(flat)
            for c in range(cuts):
                back = y[:, c * piece : (c + 1) * piece]
                answers[c, s] = (swap(back, "ep", s) if s else back).reshape(tp_n, cap, piece)
        answers = {
            c: jnp.stack([answers[c, s] for s in range(ep_n)], axis=1) for c in range(cuts)
        }
    else:
        part = jnp.stack([parcels[j] for j in order], axis=1)
        got = lax.all_to_all(part, "ep", split_axis=0, concat_axis=0, tiled=True)
        y = expert(got.reshape(-1, model)).reshape(got.shape)
        back = lax.all_to_all(y, "ep", split_axis=0, concat_axis=0, tiled=True)
        back = jnp.swapaxes(back, 0, 1)
        answers = {c: back[..., c * piece : (c + 1) * piece] for c in range(cuts)}

    places = (z * span + jnp.arange(span, dtype=jnp.int32)).astype(F32)
    frequency = ROPE_BASE ** (-jnp.arange(half, dtype=F32) / half)
    angles = places[:, None] * jnp.tile(frequency, width // half)[None, :]
    local_out, lift, packed = call(
        functools.partial(local_kernel, heads),
        (
            jax.ShapeDtypeStruct((span, heads * dv), F32),
            jax.ShapeDtypeStruct((span, width), BF16),
            jax.ShapeDtypeStruct((width + 16, dv), BF16),
        ),
        2_000_000_000, 2_000_000,
        queries, keys, values, log_decay.T, angles,
    )
    state_in = jnp.zeros((width, dv), F32)
    since = jnp.zeros((width,), F32)
    if direct:
        earlier = [
            lax.ppermute(packed, "ep", [(i, i + s) for i in range(ep_n - s)])
            for s in range(1, ep_n)
        ]
    else:
        every = lax.all_gather(packed, "ep")
        earlier = [
            jnp.where(
                z >= s, lax.dynamic_index_in_dim(every, jnp.maximum(z - s, 0), 0, False), 0
            ).astype(BF16)
            for s in range(1, ep_n)
        ]
    for got in earlier:
        got = got.astype(F32)
        state_in = state_in + jnp.exp(since)[:, None] * got[:width]
        since = since + (got[width] + got[width + 8])
    mixed = call(
        functools.partial(finish_kernel, heads),
        jax.ShapeDtypeStruct((span, w_out.shape[1]), BF16),
        4_000_000_000, 4_000_000,
        local_out, lift, state_in.astype(BF16), gate, w_out,
    )
    mixed = mixed.reshape(tp_n, span // tp_n, -1)
    mix_parts = {
        j: lax.dynamic_index_in_dim(mixed, t ^ j, 0, False) for j in range(tp_n)
    }
    mixer_out = scatter_rel(mix_parts, "tp").astype(BF16)

    hidden = {}
    for j in order:
        g = jnp.dot(blocks[j], shared_gate, preferred_element_type=F32)
        u = jnp.dot(blocks[j], shared_up, preferred_element_type=F32)
        hidden[j] = (jax.nn.silu(g) * u).astype(BF16)
    outs = []
    for c in range(cuts):
        parts = {}
        for i, j in enumerate(order):
            down = shared_down[:, c * piece : (c + 1) * piece]
            mine = jnp.dot(hidden[j], down, preferred_element_type=F32)
            routed = lax.dot_general(
                weights[j].reshape(ep_n * cap, rows),
                answers[c][i].reshape(ep_n * cap, piece),
                (((0,), (0,)), ((), ())),
                preferred_element_type=F32,
            )
            parts[j] = mine + routed
        outs.append(scatter_rel(parts, "tp").astype(BF16))
    return mixer_out, jnp.concatenate(outs, axis=1)


def solution(mesh):
    in_specs = (
        P(("grp", "ep"), "tp"),
        P(("grp", "ep"), "tp"),
        P(("grp", "ep"), "tp"),
        P(("grp", "ep"), "tp"),
        P(("grp", "ep"), "tp"),
        P("tp", None),
        P(("grp", "ep", "tp"), None),
        P(),
        P(("grp", "ep", "tp"), None),
        P(("grp", "ep", "tp"), None),
        P(("ep", "tp"), None, None),
        P(("ep", "tp"), None, None),
        P(("ep", "tp"), None, None),
        P(None, "tp"),
        P(None, "tp"),
        P("tp", None),
    )
    out_specs = (P(("grp", "ep", "tp"), None), P(("grp", "ep", "tp"), None))
    return jax.shard_map(
        per_device, mesh=mesh, in_specs=in_specs, out_specs=out_specs, check_vma=False
    )
```

```python
import functools

import jax
import jax.numpy as jnp
import numpy as np
from jax import lax
from jax.experimental import pallas as pl
from jax.experimental.pallas import tpu as pltpu
from jax.sharding import PartitionSpec as P

BLOCK = 128
ROPE_BASE = 10000.0
GROUP_EPS = 1e-05
NORM_EPS = 1e-06
DIRECT = 8
F32 = jnp.float32
BF16 = jnp.bfloat16


def swap(x, axis, bit):
    n = lax.axis_size(axis)
    return lax.ppermute(x, axis, [(i, i ^ bit) for i in range(n)])


def bits_of(n):
    assert n & (n - 1) == 0
    return [1 << i for i in range(n.bit_length() - 1)]


def gather_rel(x, axis):
    blocks = {0: x}
    for bit in reversed(bits_of(lax.axis_size(axis))):
        blocks.update({rel ^ bit: swap(blk, axis, bit) for rel, blk in list(blocks.items())})
    return blocks


def scatter_rel(parts, axis):
    parts = dict(parts)
    for bit in bits_of(lax.axis_size(axis)):
        for rel in [r for r in parts if r & bit]:
            got = swap(parts.pop(rel).astype(BF16), axis, bit)
            parts[rel ^ bit] = parts[rel ^ bit].astype(F32) + got.astype(F32)
    return parts[0]


def rope(x, angles, half):
    lanes = x.shape[1]
    row = lax.broadcasted_iota(jnp.int32, (lanes, lanes), 0)
    col = lax.broadcasted_iota(jnp.int32, (lanes, lanes), 1)
    low = (col % (2 * half)) < half
    turn = jnp.where(
        low & (row == col + half), -1.0, jnp.where((~low) & (row == col - half), 1.0, 0.0)
    ).astype(BF16)
    other = jnp.dot(x, turn, preferred_element_type=F32)
    return x.astype(F32) * jnp.cos(angles) + other * jnp.sin(angles)


def local_kernel(
    heads, q_ref, k_ref, v_ref, d_ref, a_ref, out_ref, lift_ref, state_ref, offset=None
):
    span, width = q_ref.shape
    dk = width // heads
    dv = v_ref.shape[1] // heads
    angles = a_ref[...]
    if offset is not None:
        place = offset + lax.broadcasted_iota(jnp.int32, (span, width), 0)
        angles = place.astype(F32) * angles
    q = rope(q_ref[...], angles, dk // 2).astype(BF16)
    k = (rope(k_ref[...], angles, dk // 2) * dk**-0.5).astype(BF16)
    row = lax.broadcasted_iota(jnp.int32, (BLOCK, BLOCK), 0)
    col = lax.broadcasted_iota(jnp.int32, (BLOCK, BLOCK), 1)
    lower = row >= col
    tri = lower.astype(F32)
    lane = lax.broadcasted_iota(jnp.int32, (BLOCK, width), 1)
    dlane = lax.broadcasted_iota(jnp.int32, (heads, width), 1)
    drow = lax.broadcasted_iota(jnp.int32, (heads, width), 0)
    spread = (dlane // dk == drow).astype(F32)
    state = [jnp.zeros((width, dv), F32) for _ in range(heads)]
    past = jnp.zeros((1, width), F32)
    for b in range(span // BLOCK):
        rows = pl.ds(b * BLOCK, BLOCK)
        at = slice(b * BLOCK, (b + 1) * BLOCK)
        qb, kb = q[at], k[at]
        wide = lax.dot_general(d_ref[:, rows], spread, (((0,), (0,)), ((), ())), precision=lax.Precision.HIGHEST,
                       preferred_element_type=F32)
        run = jnp.dot(tri, wide, precision=lax.Precision.HIGHEST, preferred_element_type=F32)
        last = run[BLOCK - 1 : BLOCK, :]
        lifted = (qb.astype(F32) * jnp.exp(run)).astype(BF16)
        lift_ref[rows, :] = (qb.astype(F32) * jnp.exp(run + past)).astype(BF16)
        tail = (kb.astype(F32) * jnp.exp(last - run)).astype(BF16)
        run_t = run.T
        for h in range(heads):
            mine = lane // dk == h
            zero = jnp.zeros((), BF16)
            qh = jnp.where(mine, qb, zero)
            vb = v_ref[rows, h * dv : (h + 1) * dv]
            scores = lax.dot_general(qh, kb, (((1,), (1,)), ((), ())), preferred_element_type=F32)
            gap = run[:, h * dk : h * dk + 1] - run_t[h * dk : h * dk + 1, :]
            w = jnp.where(lower, scores * jnp.exp(jnp.where(lower, gap, 0.0)), 0.0).astype(BF16)
            out = jnp.dot(w, vb, preferred_element_type=F32)
            if b:
                lh = jnp.where(mine, lifted, zero)
                out = out + jnp.dot(lh, state[h].astype(BF16), preferred_element_type=F32)
            out_ref[rows, h * dv : (h + 1) * dv] = out
            th = jnp.where(mine, tail, zero)
            grown = lax.dot_general(th, vb, (((0,), (0,)), ((), ())), preferred_element_type=F32)
            state[h] = state[h] * jnp.exp(last[:, h * dk : h * dk + 1]) + grown
        past = past + last
    total = state[0]
    for h in range(1, heads):
        total = total + state[h]
    state_ref[:width, :] = total.astype(BF16)
    hi = past.astype(BF16)
    lo = (past - hi.astype(F32)).astype(BF16)
    pad = 8
    state_ref[width : width + pad, :] = jnp.broadcast_to(hi, (pad, width))
    state_ref[width + pad :, :] = jnp.broadcast_to(lo, (pad, width))


def finish_kernel(heads, out_ref, lift_ref, state_ref, gate_ref, w_ref, mix_ref):
    width = lift_ref.shape[1]
    dk = width // heads
    dv = out_ref.shape[1] // heads
    lane = lax.broadcasted_iota(jnp.int32, (BLOCK, width), 1)

    def one(b, carry):
        rows = pl.ds(pl.multiple_of(b * BLOCK, BLOCK), BLOCK)
        lift = lift_ref[rows, :]
        total = jnp.zeros((BLOCK, w_ref.shape[1]), F32)
        for h in range(heads):
            lh = jnp.where(lane // dk == h, lift, jnp.zeros((), BF16))
            r = out_ref[rows, h * dv : (h + 1) * dv] + jnp.dot(
                lh, state_ref[...], preferred_element_type=F32
            )
            r = r - jnp.mean(r, axis=-1, keepdims=True)
            r = r * lax.rsqrt(jnp.mean(r * r, axis=-1, keepdims=True) + GROUP_EPS)
            g = gate_ref[rows, h * dv : (h + 1) * dv].astype(F32)
            y = (g * jax.nn.sigmoid(g) * r).astype(BF16)
            total = total + jnp.dot(
                y, w_ref[h * dv : (h + 1) * dv, :], preferred_element_type=F32
            )
        mix_ref[rows, :] = total.astype(BF16)
        return carry

    lax.fori_loop(0, out_ref.shape[0] // BLOCK, one, 0)


def call(kernel, out_shape, flops, moved, *args):
    vmem = pl.BlockSpec(memory_space=pltpu.VMEM)
    return pl.pallas_call(
        kernel,
        out_shape=out_shape,
        in_specs=[vmem] * len(args),
        out_specs=jax.tree.map(lambda _: vmem, out_shape),
        cost_estimate=pl.CostEstimate(flops=flops, bytes_accessed=moved, transcendentals=0),
        compiler_params=pltpu.CompilerParams(vmem_limit_bytes=32 << 20),
    )(*args)


def semaphores(cuts, subs):
    sizes = dict(
        meta=3, rows=5, state=3, near=2, fmeta=4, mix=2, mix2=cuts, nback=2 * cuts,
        first=2 * cuts, second=cuts, dense=4 * subs, far=8 * subs, back=16 * subs,
        pass_on=4 * subs, fin=2 * subs, fpass=2 * subs,
    )
    base, total = {}, 0
    for name, size in sizes.items():
        base[name] = total
        total += size
    return base, total


SENDS = 192
PASSED = (0, )
FIRST = 2


class At:
    def __init__(self, ref):
        self.ref = ref

    def __getitem__(self, index):
        return self.ref, index


def mega_kernel(
    dims,
    q_hbm, k_hbm, v_hbm, gate_hbm, d_ref, f_ref, x_hbm, gain_ref, route_ref, weigh_ref,
    wo_hbm, eg_hbm, eu_hbm, ed_hbm, sg_hbm, su_hbm, sd_hbm,
    mix_out, moe_out,
    lout, lift, spack, srecv, nbuf, mbuf, fmeta, fbuf, pfar, afar, yfar, pass_buf, ycomb, dsend, fin, fpass,
    wfar, pfar_pick, stbuf, sumbuf, hnear, psendn, parrn, ysendn, yrecv, wbuf, hbuf,
    mpart, mrecv, opart, orecv, wo, eg, eu, ed, sg, su, sd,
    q_ref, k_ref, v_ref, gate_ref, x_ref, send_sem, recv_sem, local_sem,
):
    heads, ep_n, tp_n, cap, top, cuts, subs = dims
    z, t = lax.axis_index("ep"), lax.axis_index("tp")
    rows, model = x_ref.shape
    span, width = q_ref.shape
    piece = model // cuts
    part_w = model // (2 * subs)
    pair = 2 * cap
    half_n = tp_n // 2
    bits = bits_of(tp_n)
    sems, _ = semaphores(cuts, subs)

    core = lax.rem(t, 2)
    cx = [core, 1 - core]
    line = t - core
    tps = [t, line + 1 - core, tp_n - 2 - line + core, tp_n - 1 - t]
    ends = [line, line + 1]
    side = z // 2
    near = z + 1 - 2 * lax.rem(z, 2)
    inner = (z == 1) | (z == 2)
    outer = jnp.logical_not(inner)
    relay = 2 - side
    near_peer = {"ep": near}
    crossing = {"ep": relay}

    barrier = pltpu.get_barrier_semaphore()
    for s in range(ep_n):
        for r in range(tp_n):
            if s or r:
                pl.semaphore_signal(
                    barrier, 1, device_id={"ep": lax.rem(z + s, ep_n), "tp": tps[r]}
                )

    early = []
    for i, (a, b) in enumerate(
        ((x_hbm, x_ref), (q_hbm, q_ref), (k_hbm, k_ref), (v_hbm, v_ref), (gate_hbm, gate_ref))
    ):
        early.append(pltpu.make_async_copy(a, b, local_sem.at[7 + i]))
        early[-1].start()
    loads = []
    for i, (a, b) in enumerate(
        ((sg_hbm, sg), (su_hbm, su), (eg_hbm.at[0], eg), (eu_hbm.at[0], eu),
         (ed_hbm.at[0], ed), (wo_hbm, wo), (sd_hbm, sd))
    ):
        loads.append(pltpu.make_async_copy(a, b, local_sem.at[i]))
        loads[-1].start()
    mbuf[0, :top, :] = route_ref[...].astype(F32)
    mbuf[0, top : 2 * top, :] = weigh_ref[...]
    mbuf[0, 2 * top :, :] = jnp.zeros((8 - 2 * top, rows), F32)

    early[0].wait()
    src = x_ref[...].astype(F32)
    scale = lax.rsqrt(jnp.mean(src * src, axis=-1, keepdims=True) + NORM_EPS)
    nbuf[:rows, :] = (src * scale * gain_ref[...]).astype(BF16)
    for s in range(1, ep_n):
        @pl.when(z < s)
        def _():
            srecv[s] = jnp.zeros(srecv.shape[1:], BF16)
    pl.semaphore_wait(barrier, ep_n * tp_n - 1)

    started = []

    def describe(k, i, src, dst, peer):
        src, dst = (r[0].at[r[1]] if isinstance(r, tuple) else r for r in (src, dst))
        return pltpu.make_async_remote_copy(
            src_ref=src, dst_ref=dst, send_sem=send_sem.at[k], recv_sem=recv_sem.at[i],
            device_id=peer,
        )

    only = []

    def when(here):
        if not only:
            return pl.when(here)
        return lambda body: body() if only[-1] is here else None

    def go(i, src, dst, peer, who=None):
        who = only[-1] if only and who is None else who
        job = (len(started), i, src, dst, peer)
        describe(*job).start()
        started.append((job, who))

    def arrived(i, dst):
        describe(0, i, dst, dst, near_peer).wait_recv()

    def block(rel):
        return pl.ds(rel * rows, rows)

    def send_dense(f, sub, who):
        for ch in range(2):
            cols = pl.ds((ch * subs + sub) * part_w, part_w)
            go(
                dense_sem[f][sub], At(nbuf)[block(0), cols], At(fbuf)[f, sub, own_rows],
                {"ep": relay, "tp": ends[ch]}, who,
            )

    own_rows = pl.ds(pl.multiple_of(core * rows, rows), rows)
    dense_sem = [
        [sems["dense"] + 2 * f * subs + core * subs + sub for sub in range(subs)] for f in range(2)
    ]
    fmeta_sem = [sems["fmeta"] + 2 * f + core for f in range(2)]
    mine = [core * subs + sub for sub in range(subs)]
    fin_sem = [sems["fin"] + m for m in mine]
    cross = [[cx[c] * subs + sub for sub in range(subs)] for c in range(2)]
    one, two = {"tp": tps[1]}, {"tp": tps[2]}

    go(sems["meta"], At(mbuf)[0], At(mbuf)[1], one)
    go(sems["rows"], At(nbuf)[block(0)], At(nbuf)[block(1)], one)
    go(sems["meta"] + 1, At(mbuf)[0], At(mbuf)[2], two)
    halves = [pl.ds(h * (model // 2), model // 2) for h in range(2)]
    for h in range(2):
        go(sems["rows"] + 1 + h, At(nbuf)[block(0), halves[h]], At(nbuf)[block(2), halves[h]], two)
    for f, here in ((0, inner), (1, outer)):
        @pl.when(here)
        def _():
            for ch in range(2):
                go(
                    fmeta_sem[f], At(mbuf)[0], At(fmeta)[f, core],
                    {"ep": relay, "tp": ends[ch]}, here,
                )
            if f == 1:
                for sub in range(FIRST):
                    send_dense(f, sub, here)

    lane = lax.broadcasted_iota(jnp.int32, (rows, rows), 1)
    sub_i = lax.broadcasted_iota(jnp.int32, (rows, rows), 0)
    before = (sub_i < lane).astype(BF16)
    slot_id = lax.broadcasted_iota(jnp.int32, (cap, rows), 0).astype(F32)
    blank = jnp.zeros((cap, rows), F32)
    index = lax.broadcasted_iota(jnp.int32, (8, rows), 0)

    def plan(metas, experts):
        names = jnp.full((8, rows), -1, jnp.int32)
        for i, e in enumerate(experts):
            names = jnp.where(index == i, e, names)
        names = names.astype(F32)
        ranks, weights = [], []
        for m in metas:
            hit = [m[k : k + 1, :] == names for k in range(top)]
            mark = functools.reduce(jnp.logical_or, hit)
            weights.append(
                sum(jnp.where(hit[k], m[top + k : top + k + 1, :], 0.0) for k in range(top))
            )
            rank = jnp.dot(
                mark.astype(F32).astype(BF16), before, preferred_element_type=F32
            )
            ranks.append(jnp.where(mark, rank, -1.0))
        picks, scaled = [], []
        for i in range(len(experts)):
            for s in range(2):
                at = jnp.where(slot_id == ranks[s][i : i + 1, :], 1.0, 0.0)
                heavy = at * weights[s][i : i + 1, :]
                picks.append(jnp.concatenate([blank, at] if s else [at, blank], axis=1))
                scaled.append(jnp.concatenate([blank, heavy] if s else [heavy, blank], axis=1))
        return (
            jnp.concatenate(picks, axis=0).astype(BF16),
            jnp.concatenate(scaled, axis=0).astype(BF16),
        )

    def route(g):
        pick, scaled = plan(
            [mbuf[2 * g], mbuf[2 * g + 1]], [z * tp_n + t, near * tp_n + t]
        )
        wbuf[g] = scaled
        sent = jnp.dot(
            pick, nbuf[2 * g * rows : (2 * g + 2) * rows, :], preferred_element_type=F32
        ).astype(BF16)
        psendn[g] = sent[pair:]
        parrn[0, g] = sent[:pair]
        go(sems["near"] + g, At(psendn)[g], At(parrn)[1, g], near_peer)

    def first_rows():
        arrived(sems["meta"], At(mbuf)[1])
        arrived(sems["rows"], At(nbuf)[block(1)])
        route(0)

    def alone(here, step, *args):
        @pl.when(here)
        def _():
            only.append(here)
            step(*args)
            only.pop()

    def early_dense(sub):
        @when(inner)
        def _():
            send_dense(0, sub, inner)

    def late_dense(sub):
        @when(outer)
        def _():
            send_dense(1, sub, outer)

    def local():
        for load in early[1:]:
            load.wait()
        local_kernel(heads, q_ref, k_ref, v_ref, d_ref, f_ref, lout, lift, spack, z * span)

    def states():
        for s in range(1, ep_n - 1):
            later = z + s < ep_n - 1
            after = {"ep": lax.rem(z + s, ep_n)}

            @pl.when(later)
            def _():
                go(sems["state"] + s, spack, At(srecv)[s], after, later)

    def shared(j):
        if j == 0:
            loads[0].wait()
            loads[1].wait()
        x = nbuf[block(j), :]
        g = jnp.dot(x, sg[...], preferred_element_type=F32)
        u = jnp.dot(x, su[...], preferred_element_type=F32)
        hbuf[block(j), :] = (g * jax.nn.sigmoid(g) * u).astype(BF16)

    ends_here = z == ep_n - 1
    hands_on = z == ep_n - 2
    next_peer = {"ep": lax.rem(z + 1, ep_n)}

    def gather_states():
        for s in range(1, ep_n - 1):
            @pl.when((z >= s) & (z < ep_n - 1))
            def _():
                arrived(sems["state"] + s, At(srecv)[s])

        @pl.when(ends_here)
        def _():
            arrived(sems["state"], At(srecv)[1, pl.ds(0, width)])

        state_in = jnp.zeros((width, width), F32)
        since = jnp.zeros((8, width), F32)
        for s in range(1, ep_n):
            got = srecv[s].astype(F32)
            state_in = state_in + jnp.exp(since).T[:, :1] * got[:width]
            since = since + (got[width : width + 8] + got[width + 8 :])
        stbuf[...] = state_in.astype(BF16)
        if not only or only[-1] is inner:
            @pl.when(hands_on)
            def _():
                own = spack[...].astype(F32)
                past = own[width : width + 8] + own[width + 8 :]
                total = own[:width] + jnp.exp(past).T[:, :1] * stbuf[...].astype(F32)
                sumbuf[...] = total.astype(BF16)
                go(sems["state"], sumbuf, At(srecv)[1, pl.ds(0, width)], next_peer, hands_on)

        loads[5].wait()

    def peer_of(j):
        peer = t
        for bit in bits:
            on = lax.rem(j // bit, 2)
            peer = peer + on * (bit - 2 * bit * lax.rem(t // bit, 2))
        return peer

    def finish(first):
        def one_block(i, c):
            j = 2 * i + first
            own = pl.multiple_of(peer_of(j) * (span // tp_n), BLOCK)
            finish_rows(
                heads, lout, lift, stbuf[...], gate_ref, wo, pl.ds(own, span // tp_n), mpart, j
            )
            return c

        lax.fori_loop(0, half_n, one_block, 0)
        if first:
            for i in range(half_n):
                go(sems["mix"] + i, At(mpart)[2 * i + 1], At(mrecv)[i], one)

    def second_rows(h):
        if h == 0:
            arrived(sems["meta"] + 1, At(mbuf)[2])
            go(sems["meta"] + 2, At(mbuf)[2], At(mbuf)[3], one)
        arrived(sems["rows"] + 1 + h, At(nbuf)[block(2), halves[h]])
        go(sems["rows"] + 3 + h, At(nbuf)[block(2), halves[h]], At(nbuf)[block(3), halves[h]], one)

    def mix_add():
        for i in reversed(range(half_n)):
            arrived(sems["mix"] + i, At(mrecv)[i])
            mpart[2 * i] = (mpart[2 * i].astype(F32) + mrecv[i].astype(F32)).astype(BF16)

    def mix_piece(c, who=None):
        cols = pl.ds(c * piece, piece)
        go(sems["mix2"] + c, At(mpart)[2, :, cols], At(mrecv)[half_n, :, cols], two, who)

    def mix_inner(c):
        when(inner)(lambda: mix_piece(c, inner))

    def mix_outer(c):
        when(outer)(lambda: mix_piece(c, outer))

    def mix_done():
        for c in range(cuts):
            arrived(sems["mix2"] + c, At(mrecv)[half_n, :, pl.ds(c * piece, piece)])
        mix_out[...] = (mpart[0].astype(F32) + mrecv[half_n].astype(F32)).astype(BF16)

    def third_rows():
        arrived(sems["meta"] + 2, At(mbuf)[3])
        for h in range(2):
            arrived(sems["rows"] + 3 + h, At(nbuf)[block(3), halves[h]])
        route(1)

    everyone = [
        (near if i // tp_n else z) * tp_n + tps[i % tp_n] for i in range(2 * tp_n)
    ]

    def plan_far(f):
        @when(inner)
        def _():
            for s in range(2):
                arrived(sems["fmeta"] + 2 * f + s, At(fmeta)[f, s])
            pick, scaled = plan([fmeta[f, 0], fmeta[f, 1]], everyone)
            wfar[f] = scaled
            pfar_pick[f] = pick

    def relay_far(f, sub):
        @when(inner)
        def _():
            for s in range(2):
                arrived(sems["dense"] + (2 * f + s) * subs + sub, At(fbuf)[f, sub, block(s)])
            pfar[f, sub] = jnp.dot(
                pfar_pick[f], fbuf[f, sub], preferred_element_type=F32
            ).astype(BF16)
            for i in (6, 7, 4, 5, 2, 3, 1):
                rel = i % tp_n
                go(
                    sems["far"] + (f * subs + sub) * tp_n + rel,
                    At(pfar)[f, sub, pl.ds(i * pair, pair)],
                    At(afar)[f, mine[sub], pl.ds((rel // 2) * pair, pair)],
                    {"ep": near if i // tp_n else z, "tp": tps[rel]}, inner,
                )
            afar[f, mine[sub], :pair] = pfar[f, sub, :pair]

    def hidden(x):
        g = jnp.dot(x, eg[...], preferred_element_type=F32)
        u = jnp.dot(x, eu[...], preferred_element_type=F32)
        return (g * jax.nn.sigmoid(g) * u).astype(BF16)

    def weights():
        for i in (2, 3, 4):
            loads[i].wait()

    def near_hidden():
        for g in range(2):
            arrived(sems["near"] + g, At(parrn)[1, g])
        hnear[...] = hidden(
            jnp.concatenate([parrn[s, g] for s in range(2) for g in range(2)], axis=0)
        )

    def near_out(c):
        at = slice(c * piece, (c + 1) * piece)
        cols = pl.ds(c * piece, piece)
        y = jnp.dot(hnear[...], ed[:, at], preferred_element_type=F32).astype(BF16)
        ysendn[:, at] = y[2 * pair :]
        for g in range(2):
            yrecv[g, :pair, at] = y[g * pair : (g + 1) * pair]
            go(
                sems["nback"] + 2 * c + g, At(ysendn)[pl.ds(g * pair, pair), cols],
                At(yrecv)[g, pl.ds(pair, pair), cols], near_peer,
            )

    def experts_far(f):
        for sub in range(subs):
            for rel in range(tp_n):
                i = sems["far"] + (f * subs + sub) * tp_n + rel
                dst = At(afar)[f, cross[rel % 2][sub], pl.ds((rel // 2) * pair, pair)]
                if rel:
                    arrived(i, dst)
                else:
                    @when(outer)
                    def _():
                        arrived(i, dst)
        h = hidden(jnp.concatenate([afar[f, q] for q in range(2 * subs)], axis=1))
        for sub in range(subs):
            for ch in range(2):
                q = ch * subs + sub
                yfar[f, q] = jnp.dot(
                    h, ed[:, q * part_w : (q + 1) * part_w], preferred_element_type=F32
                ).astype(BF16)
            base = sems["back"] + (f * subs + sub) * 2 * tp_n

            @when(inner)
            def _():
                for rel in (2, 3, 1):
                    go(
                        base + rel,
                        At(yfar)[f, cross[rel % 2][sub], pl.ds((rel // 2) * pair, pair)],
                        At(ycomb)[f, sub, pl.ds(rel * pair, pair)], {"tp": tps[rel]}, inner,
                    )
                ycomb[f, sub, :pair] = yfar[f, mine[sub], :pair]

            @when(outer)
            def _():
                if f in PASSED:
                    for ch in range(2):
                        q = ch * subs + sub
                        go(
                            sems["pass_on"] + f * 2 * subs + q,
                            At(yfar)[f, q, pl.ds(pair, pair)], At(pass_buf)[f, q], two, outer,
                        )
                for rel in (0, 1) if f in PASSED else (2, 3, 0, 1):
                    go(
                        base + tp_n + rel,
                        At(yfar)[f, cross[rel % 2][sub], pl.ds((rel // 2) * pair, pair)],
                        At(ycomb)[f, sub, pl.ds((tp_n + rel) * pair, pair)],
                        {"ep": near, "tp": tps[rel]}, outer,
                    )

    def pass_far(f, sub):
        @when(outer)
        def _():
            for ch in range(2):
                q = ch * subs + sub
                arrived(sems["pass_on"] + f * 2 * subs + q, At(pass_buf)[f, q])
            for c in range(2):
                go(
                    sems["back"] + (f * subs + sub) * 2 * tp_n + tp_n + 2 + c,
                    At(pass_buf)[f, cross[c][sub]],
                    At(ycomb)[f, sub, pl.ds((tp_n + 2 + c) * pair, pair)],
                    {"ep": near, "tp": tps[c]}, outer,
                )

    def combine_far(f, sub):
        @when(inner)
        def _():
            for i in range(1, 2 * tp_n):
                arrived(
                    sems["back"] + (f * subs + sub) * 2 * tp_n + i,
                    At(ycomb)[f, sub, pl.ds(i * pair, pair)],
                )
            dsend[f, sub] = lax.dot_general(
                wfar[f], ycomb[f, sub], (((0,), (0,)), ((), ())), preferred_element_type=F32
            ).astype(BF16)
            for s in range(2):
                if f:
                    go(
                        sems["fpass"] + 2 * sub + s, At(dsend)[f, sub, block(s)],
                        At(fpass)[sub, block(s)], crossing, inner,
                    )
                else:
                    go(
                        fin_sem[sub], At(dsend)[f, sub, block(s)], At(fin)[mine[sub]],
                        {"ep": relay, "tp": ends[s]}, inner,
                    )

    def pass_fin(sub):
        @when(inner)
        def _():
            for s in range(2):
                arrived(sems["fpass"] + 2 * sub + s, At(fpass)[sub, block(s)])
                go(
                    fin_sem[sub], At(fpass)[sub, block(s)], At(fin)[mine[sub]],
                    {"ep": near, "tp": ends[s]}, inner,
                )

    def combine_near(c):
        if c == 0:
            loads[6].wait()
        at = slice(c * piece, (c + 1) * piece)
        cols = pl.ds(c * piece, piece)
        for g in range(2):
            arrived(sems["nback"] + 2 * c + g, At(yrecv)[g, pl.ds(pair, pair), cols])
        for g in (1, 0):
            part = lax.dot_general(
                wbuf[g], yrecv[g, :, at], (((0,), (0,)), ((), ())), preferred_element_type=F32
            )
            part = part + jnp.dot(
                hbuf[2 * g * rows : (2 * g + 2) * rows, :], sd[:, at], preferred_element_type=F32
            )
            opart[2 * g + 1, :, at] = part[rows:].astype(BF16)
            go(
                sems["first"] + 2 * c + g, At(opart)[2 * g + 1, :, cols],
                At(orecv)[g, :, cols], one,
            )
            opart[2 * g, :, at] = part[:rows].astype(BF16)

    def second(c):
        at = slice(c * piece, (c + 1) * piece)
        cols = pl.ds(c * piece, piece)
        for g in (1, 0):
            arrived(sems["first"] + 2 * c + g, At(orecv)[g, :, cols])
            opart[2 * g, :, at] = (
                opart[2 * g, :, at].astype(F32) + orecv[g, :, at].astype(F32)
            ).astype(BF16)
            if g:
                go(sems["second"] + c, At(opart)[2, :, cols], At(orecv)[2, :, cols], two)

    def moe_done():
        for c in range(cuts):
            arrived(sems["second"] + c, At(orecv)[2, :, pl.ds(c * piece, piece)])
        for sub in range(subs):
            for ch in range(2):
                q = ch * subs + sub
                at = slice(q * part_w, (q + 1) * part_w)
                arrived(sems["fin"] + q, At(fin)[q])
                moe_out[:, at] = (
                    opart[0, :, at].astype(F32) + orecv[2, :, at].astype(F32)
                    + fin[q].astype(F32)
                ).astype(BF16)

    early_sends = [0]

    def flush(jobs):
        for job, who in jobs:
            if who is None:
                describe(*job).wait_send()
        conditions = []
        for _, who in jobs:
            if who is not None and all(who is not w for w in conditions):
                conditions.append(who)
        for w in conditions:
            @pl.when(w)
            def _():
                for job, who in jobs:
                    if who is w:
                        describe(*job).wait_send()

    def mark():
        early_sends[0] = len(started)

    def drain():
        flush(started[: early_sends[0]])

    local()
    states()
    early_dense(0)
    early_dense(1)
    first_rows()
    plan_far(1)
    shared(0)
    shared(1)
    relay_far(1, 0)
    second_rows(0)
    relay_far(1, 1)
    second_rows(1)
    third_rows()
    plan_far(0)
    alone(inner, gather_states)
    alone(inner, finish, 1)
    alone(inner, finish, 0)
    alone(inner, mix_add)
    relay_far(0, 0)
    weights()
    experts_far(1)
    alone(outer, near_hidden)
    alone(outer, near_out, 0)
    alone(outer, near_out, 1)
    alone(outer, near_out, 2)
    alone(outer, near_out, 3)
    alone(outer, gather_states)
    alone(outer, finish, 1)
    alone(outer, finish, 0)
    alone(outer, mix_add)
    mix_outer(0)
    mix_outer(1)
    alone(outer, shared, 2)
    alone(outer, shared, 3)
    alone(outer, experts_far, 0)
    mix_outer(2)
    mix_outer(3)
    pass_far(0, 0)
    pass_far(0, 1)
    relay_far(0, 1)
    mix_inner(0)
    alone(inner, near_hidden)
    alone(inner, near_out, 0)
    alone(inner, near_out, 1)
    alone(inner, near_out, 2)
    alone(inner, near_out, 3)
    alone(inner, shared, 2)
    alone(inner, shared, 3)
    combine_far(1, 0)
    combine_far(1, 1)
    mix_inner(1)
    alone(inner, experts_far, 0)
    mix_inner(2)
    mix_inner(3)
    mark()
    combine_near(0)
    combine_near(1)
    second(0)
    second(1)
    pass_fin(0)
    combine_far(0, 0)
    combine_far(0, 1)
    pass_fin(1)
    combine_near(2)
    combine_near(3)
    second(2)
    second(3)
    drain()
    mix_done()
    moe_done()

    flush(started[early_sends[0] :])
    assert len(started) <= SENDS


def finish_rows(heads, lout, lift_ref, state, gate_ref, wo, at, mpart, j):
    width = lift_ref.shape[1]
    dk = width // heads
    dv = lout.shape[1] // heads
    lift = lift_ref[at, :]
    lane = lax.broadcasted_iota(jnp.int32, lift.shape, 1)
    ys = []
    for h in range(heads):
        lh = jnp.where(lane // dk == h, lift, jnp.zeros((), BF16))
        r = lout[at, h * dv : (h + 1) * dv] + jnp.dot(lh, state, preferred_element_type=F32)
        r = r - jnp.mean(r, axis=-1, keepdims=True)
        r = r * lax.rsqrt(jnp.mean(r * r, axis=-1, keepdims=True) + GROUP_EPS)
        g = gate_ref[at, h * dv : (h + 1) * dv].astype(F32)
        ys.append((g * jax.nn.sigmoid(g) * r).astype(BF16))
    y = jnp.concatenate(ys, axis=1)
    mpart[j] = jnp.dot(y, wo[...], preferred_element_type=F32).astype(BF16)


def mega(
    queries, keys, values, gate, log_decay, w_out, moe_input, moe_gain, routes, route_weight,
    expert_gate, expert_up, expert_down, shared_gate, shared_up, shared_down,
):
    span, width = queries.shape
    heads = log_decay.shape[1]
    half = width // heads // 2
    rows, model = moe_input.shape
    top = routes.shape[1]
    ep_n, tp_n = lax.axis_size("ep"), lax.axis_size("tp")
    cap = rows * top * 3 // (2 * ep_n * tp_n)
    pair, cuts, subs = 2 * cap, 4, 2
    steps = np.arange(half, dtype=np.float32) / np.float32(half)
    freq = np.power(np.float32(ROPE_BASE), -steps).astype(np.float32)
    freq = jnp.asarray(np.tile(freq, width // half)[None, :])
    vmem = pl.BlockSpec(memory_space=pltpu.VMEM)
    hbm = pl.BlockSpec(memory_space=pl.ANY)
    V = pltpu.VMEM
    half_n = tp_n // 2
    part_w = model // (2 * subs)
    copies = semaphores(cuts, subs)[1]
    return pl.pallas_call(
        functools.partial(mega_kernel, (heads, ep_n, tp_n, cap, top, cuts, subs)),
        out_shape=(V((rows, w_out.shape[1]), BF16), V((rows, model), BF16)),
        in_specs=[hbm] * 4 + [vmem] * 2 + [hbm] + [vmem] * 3 + [hbm] * 7,
        out_specs=(vmem, vmem),
        scratch_shapes=[
            V((span, values.shape[1]), F32), V((span, width), BF16),
            V((width + 16, width), BF16), V((ep_n, width + 16, width), BF16),
            V((tp_n * rows, model), BF16), V((tp_n, 8, rows), F32),
            V((2, 2, 8, rows), F32), V((2, subs, 2 * rows, part_w), BF16),
            V((2, subs, 2 * tp_n * pair, part_w), BF16), V((2, 2 * subs, 2 * pair, part_w), BF16),
            V((2, 2 * subs, 2 * pair, part_w), BF16), V((2, 2 * subs, pair, part_w), BF16),
            V((2, subs, 2 * tp_n * pair, part_w), BF16), V((2, subs, 2 * rows, part_w), BF16),
            V((2 * subs, rows, part_w), BF16), V((subs, 2 * rows, part_w), BF16), V((2, 2 * tp_n * pair, 2 * rows), BF16),
            V((2, 2 * tp_n * pair, 2 * rows), BF16), V((width, width), BF16), V((width, width), BF16),
            V((4 * pair, expert_gate.shape[2]), BF16),
            V((2, pair, model), BF16), V((2, 2, pair, model), BF16),
            V((2 * pair, model), BF16), V((2, 2 * pair, model), BF16),
            V((2, 2 * pair, 2 * rows), BF16), V((tp_n * rows, shared_gate.shape[1]), BF16),
            V((tp_n, span // tp_n, w_out.shape[1]), BF16),
            V((half_n + 1, span // tp_n, w_out.shape[1]), BF16),
            V((tp_n, rows, model), BF16), V((half_n + 1, rows, model), BF16),
            V(w_out.shape, BF16), V(expert_gate.shape[1:], BF16), V(expert_up.shape[1:], BF16),
            V(expert_down.shape[1:], BF16), V(shared_gate.shape, BF16),
            V(shared_up.shape, BF16), V(shared_down.shape, BF16),
            V(queries.shape, BF16), V(keys.shape, BF16), V(values.shape, BF16), V(gate.shape, BF16),
            V(moe_input.shape, BF16),
            pltpu.SemaphoreType.DMA((SENDS,)), pltpu.SemaphoreType.DMA((copies,)),
            pltpu.SemaphoreType.DMA((12,)),
        ],
        compiler_params=pltpu.CompilerParams(
            collective_id=0, has_side_effects=True, vmem_limit_bytes=60 << 20
        ),
    )(
        queries, keys, values, gate, log_decay.T, freq, moe_input, moe_gain[None, :],
        routes.T, route_weight.T,
        w_out, expert_gate, expert_up, expert_down, shared_gate, shared_up, shared_down,
    )


def per_device(
    queries, keys, values, gate, log_decay, w_out, moe_input, moe_gain, routes, route_weight,
    expert_gate, expert_up, expert_down, shared_gate, shared_up, shared_down,
):
    span = queries.shape[0]
    heads = log_decay.shape[1]
    width = queries.shape[1]
    dk = width // heads
    half = dk // 2
    dv = values.shape[1] // heads
    rows, model = moe_input.shape
    top = routes.shape[1]
    ep_n, tp_n = lax.axis_size("ep"), lax.axis_size("tp")
    z, t = lax.axis_index("ep"), lax.axis_index("tp")
    direct = ep_n <= DIRECT and ep_n & (ep_n - 1) == 0
    if ep_n == 4 and tp_n == 4 and dv == width and (rows * top * 3 // (ep_n * tp_n)) % 16 == 0:
        return mega(
            queries, keys, values, gate, log_decay, w_out, moe_input, moe_gain, routes,
            route_weight, expert_gate, expert_up, expert_down, shared_gate, shared_up, shared_down,
        )
    cap = rows * top * 3 // (2 * ep_n * tp_n)

    source = moe_input.astype(F32)
    scale_row = lax.rsqrt(jnp.mean(source * source, axis=-1, keepdims=True) + NORM_EPS)
    normed = (source * scale_row * moe_gain[None, :]).astype(BF16)
    meta = jnp.concatenate([routes.astype(F32).T, route_weight.T], axis=0)
    blocks = gather_rel(normed, "tp")
    metas = gather_rel(meta, "tp")
    order = sorted(blocks)

    step = jnp.arange(ep_n, dtype=jnp.int32)
    peers = (z ^ step) if direct else step
    named = (peers * tp_n + t).astype(F32)
    before = (jnp.arange(rows)[:, None] < jnp.arange(rows)[None, :]).astype(BF16)
    parcels, weights = {}, {}
    for j in order:
        hits = metas[j][:top, None, :] == named[None, :, None]
        mark = jnp.any(hits, axis=0)
        weight = jnp.sum(jnp.where(hits, metas[j][top:, None, :], 0.0), axis=0)
        rank = jnp.dot(mark.astype(BF16), before, preferred_element_type=F32)
        slot = mark[:, None, :] & (rank[:, None, :] == jnp.arange(cap, dtype=F32)[None, :, None])
        pick = slot.astype(BF16).reshape(ep_n * cap, rows)
        weights[j] = jnp.where(slot, weight[:, None, :], 0.0).astype(BF16)
        parcels[j] = jnp.dot(pick, blocks[j], preferred_element_type=F32).astype(BF16).reshape(
            ep_n, cap, model
        )

    half_tp = max(1, tp_n // 2)
    groups = [order[:half_tp], order[half_tp:]] if tp_n > 1 else [order]

    def expert(x):
        g = jnp.dot(x, expert_gate[0], preferred_element_type=F32)
        u = jnp.dot(x, expert_up[0], preferred_element_type=F32)
        h = (jax.nn.silu(g) * u).astype(BF16)
        return jnp.dot(h, expert_down[0], preferred_element_type=F32).astype(BF16)

    cuts = 2
    piece = model // cuts
    answers = {}
    if direct:
        arrived = {}
        for group in groups:
            part = jnp.stack([parcels[j] for j in group], axis=1)
            for s in reversed(range(ep_n)):
                got = swap(part[s], "ep", s) if s else part[0]
                arrived.setdefault(s, []).append(got)
        for s in reversed(range(ep_n)):
            flat = jnp.concatenate(arrived[s], axis=0).reshape(tp_n * cap, model)
            y = expert(flat)
            for c in range(cuts):
                back = y[:, c * piece : (c + 1) * piece]
                answers[c, s] = (swap(back, "ep", s) if s else back).reshape(tp_n, cap, piece)
        answers = {
            c: jnp.stack([answers[c, s] for s in range(ep_n)], axis=1) for c in range(cuts)
        }
    else:
        part = jnp.stack([parcels[j] for j in order], axis=1)
        got = lax.all_to_all(part, "ep", split_axis=0, concat_axis=0, tiled=True)
        y = expert(got.reshape(-1, model)).reshape(got.shape)
        back = lax.all_to_all(y, "ep", split_axis=0, concat_axis=0, tiled=True)
        back = jnp.swapaxes(back, 0, 1)
        answers = {c: back[..., c * piece : (c + 1) * piece] for c in range(cuts)}

    places = (z * span + jnp.arange(span, dtype=jnp.int32)).astype(F32)
    frequency = ROPE_BASE ** (-jnp.arange(half, dtype=F32) / half)
    angles = places[:, None] * jnp.tile(frequency, width // half)[None, :]
    local_out, lift, packed = call(
        functools.partial(local_kernel, heads),
        (
            jax.ShapeDtypeStruct((span, heads * dv), F32),
            jax.ShapeDtypeStruct((span, width), BF16),
            jax.ShapeDtypeStruct((width + 16, dv), BF16),
        ),
        2_000_000_000, 2_000_000,
        queries, keys, values, log_decay.T, angles,
    )
    state_in = jnp.zeros((width, dv), F32)
    since = jnp.zeros((width,), F32)
    if direct:
        earlier = [
            lax.ppermute(packed, "ep", [(i, i + s) for i in range(ep_n - s)])
            for s in range(1, ep_n)
        ]
    else:
        every = lax.all_gather(packed, "ep")
        earlier = [
            jnp.where(
                z >= s, lax.dynamic_index_in_dim(every, jnp.maximum(z - s, 0), 0, False), 0
            ).astype(BF16)
            for s in range(1, ep_n)
        ]
    for got in earlier:
        got = got.astype(F32)
        state_in = state_in + jnp.exp(since)[:, None] * got[:width]
        since = since + (got[width] + got[width + 8])
    mixed = call(
        functools.partial(finish_kernel, heads),
        jax.ShapeDtypeStruct((span, w_out.shape[1]), BF16),
        4_000_000_000, 4_000_000,
        local_out, lift, state_in.astype(BF16), gate, w_out,
    )
    mixed = mixed.reshape(tp_n, span // tp_n, -1)
    mix_parts = {
        j: lax.dynamic_index_in_dim(mixed, t ^ j, 0, False) for j in range(tp_n)
    }
    mixer_out = scatter_rel(mix_parts, "tp").astype(BF16)

    hidden = {}
    for j in order:
        g = jnp.dot(blocks[j], shared_gate, preferred_element_type=F32)
        u = jnp.dot(blocks[j], shared_up, preferred_element_type=F32)
        hidden[j] = (jax.nn.silu(g) * u).astype(BF16)
    outs = []
    for c in range(cuts):
        parts = {}
        for i, j in enumerate(order):
            down = shared_down[:, c * piece : (c + 1) * piece]
            mine = jnp.dot(hidden[j], down, preferred_element_type=F32)
            routed = lax.dot_general(
                weights[j].reshape(ep_n * cap, rows),
                answers[c][i].reshape(ep_n * cap, piece),
                (((0,), (0,)), ((), ())),
                preferred_element_type=F32,
            )
            parts[j] = mine + routed
        outs.append(scatter_rel(parts, "tp").astype(BF16))
    return mixer_out, jnp.concatenate(outs, axis=1)


def solution(mesh):
    in_specs = (
        P(("grp", "ep"), "tp"),
        P(("grp", "ep"), "tp"),
        P(("grp", "ep"), "tp"),
        P(("grp", "ep"), "tp"),
        P(("grp", "ep"), "tp"),
        P("tp", None),
        P(("grp", "ep", "tp"), None),
        P(),
        P(("grp", "ep", "tp"), None),
        P(("grp", "ep", "tp"), None),
        P(("ep", "tp"), None, None),
        P(("ep", "tp"), None, None),
        P(("ep", "tp"), None, None),
        P(None, "tp"),
        P(None, "tp"),
        P("tp", None),
    )
    out_specs = (P(("grp", "ep", "tp"), None), P(("grp", "ep", "tp"), None))
    return jax.shard_map(
        per_device, mesh=mesh, in_specs=in_specs, out_specs=out_specs, check_vma=False
    )
```
